128 devices in a mesh: ra: 16 (over z, x), cb: 4 (over y), dp: 2 (over core).
Axes of the slice: x: 4, y: 4, z: 4, core: 2. Of those that a mesh axis runs over, the one named last changes fastest.
Arguments:
- tokens: bfloat16 [1024, 4096], P('dp', 'ra'), may hold values from -160 to 160, as said below
- first_gain: bfloat16 [4096], P('ra'), may hold values from 0.099609375 to 1.8984375
- first_gate: bfloat16 [4096, 6144], P('ra', 'cb'), may hold values from -0.125 to 0.125
- first_up: bfloat16 [4096, 6144], P('ra', 'cb'), may hold values from -0.125 to 0.125
- first_down: bfloat16 [6144, 4096], P(('cb', 'ra')), may hold values from -0.21875 to 0.21875
- first_branch: bfloat16 [4096], P('ra'), may hold values from 1 to 4
- second_gain: bfloat16 [4096], P('ra'), may hold values from 0.099609375 to 1.8984375
- second_gate: bfloat16 [4096, 6144], P('ra', 'cb'), may hold values from -0.125 to 0.125
- second_up: bfloat16 [4096, 6144], P('ra', 'cb'), may hold values from -0.125 to 0.125
- second_down: bfloat16 [6144, 4096], P(('cb', 'ra')), may hold values from -0.21875 to 0.21875
- second_branch: bfloat16 [4096], P('ra'), may hold values from 1 to 4
Outputs:
- mixed_out: bfloat16 [1024, 4096], P('dp', 'ra')
The draws below stay inside these ranges and needn't reach their ends.
Inputs may be any that keep to these rules, and one draw needn't show every extreme that they name: `tokens`: activations whose scale varies by token and by feature.
All inputs are finite; a program needn't handle non-finite values.
Results may differ from the reference program's by a relative error of at most 0.035.
Values may be sent and summed in bfloat16 or wider, within the bound.
No kernel may reach another device: no remote copies, remote signals or barrier semaphores. Data moves between devices by JAX's collectives and lax.ppermute only.
A program may use at most 64 MiB of HBM per device.

```python
import math
import jax
import jax.numpy as jnp
from jax import lax

D = 4096
FF = 6144
TOKENS = 1024


def draw_tokens(key, part):
    first_key, second_key, third_key = jax.random.split(jax.random.fold_in(key, 11), 3)
    columns = jnp.exp(jnp.log(6.0) * jnp.arange(D, dtype=jnp.float32) / D) * jax.random.uniform(second_key, (D,), jnp.float32, 0.5, 1.5)
    rows = jnp.exp(jax.random.uniform(third_key, (TOKENS, 1), jnp.float32, 0.0, jnp.log(4.0)))
    base = jax.random.truncated_normal(first_key, -4.0, 4.0, (TOKENS, D), jnp.float32)
    return (base * rows * columns[None, :]).astype(jnp.bfloat16)


def raised(array, rng, source, target, blocks, factor):
    def block_of(axis_at):
        return (jnp.arange(array.shape[axis_at]) // (array.shape[axis_at] // blocks)).reshape((-1,) + (1,) * (array.ndim - 1 - axis_at))

    first = jax.random.permutation(rng, blocks)[block_of(target)]
    second = (block_of(target) + blocks // 2) % blocks
    return jnp.where((block_of(source) == first) | (block_of(source) == second), factor * array, array)


def steps_of(key, shape, pieces, smallest, top_value):
    loudness = 1.0
    for dim, parts in pieces:
        draws = jax.random.uniform(jax.random.fold_in(jax.random.fold_in(key, 6), dim), (parts,), jnp.float32, smallest / len(pieces), top_value / len(pieces))
        loudness = loudness * jnp.repeat(jnp.exp(draws), shape[dim] // parts).reshape((-1,) + (1,) * (len(shape) - 1 - dim))
    return loudness


def gaussian_with(key, dims, scale, reach, shards, heavy, kind=jnp.bfloat16):
    values = scale * jax.random.normal(key, dims, jnp.float32)
    if shards:
        values = values * steps_of(key, dims, shards, -0.22, 0.18)
    return jnp.clip(raised(values, jax.random.fold_in(key, 3), *heavy), -reach, reach).astype(kind)


def setup_inputs(seed: int = 0) -> dict:
    key_of = jax.random.split(jax.random.key(seed), 12)
    return {
        "tokens": draw_tokens(jax.random.fold_in(key_of[11], 71), 0),
        "first_gain": jnp.clip(1.0 + 0.18 * jax.random.normal(key_of[1], (D,), jnp.float32), 0.099609375, 1.8984375).astype(jnp.bfloat16),
        "first_gate": gaussian_with(key_of[2], (D, FF), D ** -0.5, 0.125, ((0, 16), (1, 4)), (0, 1, 16, 2.0)),
        "first_up": gaussian_with(key_of[3], (D, FF), D ** -0.5, 0.125, ((0, 16), (1, 4)), (0, 1, 16, 2.0)),
        "first_down": gaussian_with(key_of[4], (FF, D), FF ** -0.5, 0.21875, ((0, 64),), (0, 1, 64, 4.0)),
        "first_branch": jnp.clip(jnp.exp(math.log(4.0) - 1.3862944 * jax.random.uniform(key_of[5], (D,), jnp.float32) ** steps_of(key_of[5], (D,), ((0, 16),), -0.2, 0.2)), 1.0, 4.0).astype(jnp.bfloat16),
        "second_gain": jnp.clip(1.0 + 0.18 * jax.random.normal(key_of[6], (D,), jnp.float32), 0.099609375, 1.8984375).astype(jnp.bfloat16),
        "second_gate": gaussian_with(key_of[7], (D, FF), D ** -0.5, 0.125, ((0, 16), (1, 4)), (0, 1, 16, 2.0)),
        "second_up": gaussian_with(key_of[8], (D, FF), D ** -0.5, 0.125, ((0, 16), (1, 4)), (0, 1, 16, 2.0)),
        "second_down": gaussian_with(key_of[9], (FF, D), FF ** -0.5, 0.21875, ((0, 64),), (0, 1, 64, 4.0)),
        "second_branch": jnp.clip(jnp.exp(math.log(4.0) - 1.3862944 * jax.random.uniform(key_of[10], (D,), jnp.float32) ** steps_of(key_of[10], (D,), ((0, 16),), -0.2, 0.2)), 1.0, 4.0).astype(jnp.bfloat16),
    }


epsilon = 1e-06
residual_scale = 0.25

def half_step(values, norm_gain, w_gate, w_up, w_down, branch_gain):
    wide_values = values.astype(jnp.float32)
    mean_square = lax.optimization_barrier(jnp.mean(wide_values * wide_values, axis=1, keepdims=True))
    normed = (wide_values * lax.rsqrt(mean_square + epsilon) * norm_gain.astype(jnp.float32)).astype(jnp.bfloat16)
    gate = jnp.dot(normed, w_gate, preferred_element_type=jnp.float32)
    upward = jnp.dot(normed, w_up, preferred_element_type=jnp.float32)
    hidden = (jax.nn.silu(gate) * upward).astype(jnp.bfloat16)
    branch = jnp.dot(hidden, w_down, preferred_element_type=jnp.float32)
    return (residual_scale * wide_values + 0.5 * branch_gain.astype(jnp.float32) * branch).astype(jnp.bfloat16)

def reference(tokens, first_gain, first_gate, first_up, first_down, first_branch, second_gain, second_gate, second_up, second_down, second_branch):
    middle = half_step(tokens, first_gain, first_gate, first_up, first_down, first_branch)
    return half_step(middle, second_gain, second_gate, second_up, second_down, second_branch)
```

```python
import jax
import jax.numpy as jnp
from jax import lax
from jax.sharding import Mesh, PartitionSpec as P

epsilon = 1e-06
residual_scale = 0.25
f32 = jnp.float32
bf16 = jnp.bfloat16


def exchange(x, axes):
    return lax.all_to_all(x, axes, 0, 0, tiled=True)


def to_all(x, n):
    return jnp.broadcast_to(x[None], (n, *x.shape))


def other_core(x):
    return lax.ppermute(x, "dp", [(0, 1), (1, 0)])


def shifted(x, axis, step):
    return lax.ppermute(x, axis, [(i, (i + step) % 4) for i in range(4)])


def pick(x, at):
    return lax.dynamic_index_in_dim(x, at % 4, 0, keepdims=False)


def up_weights(w_gate, w_up, core, z):
    rows, cols = w_gate.shape
    half, part = rows // 2, cols // 4
    pieces = []
    for step in range(4):
        to = (z + step) % 4
        mine = jnp.concatenate(
            [
                lax.dynamic_slice(w, (core * half, to * part), (half, part))
                for w in (w_gate, w_up)
            ],
            1,
        )
        pieces.append(shifted(mine, "rz", step) if step else mine)
    return pieces


def down_weights(w_down, core, x):
    rows, cols = w_down.shape
    mine = lax.dynamic_slice_in_dim(w_down, core * (cols // 2), cols // 2, 1)
    whole = jnp.zeros((4 * rows, cols // 2), w_down.dtype)
    for step in range(4):
        piece = shifted(mine, "rx", step) if step else mine
        whole = lax.dynamic_update_slice(whole, piece, (((x - step) % 4) * rows, 0))
    return whole


def halves_by_core(x, core):
    half = x.shape[-1] // 2
    a, b = x[..., :half], x[..., half:]
    first = core == 0
    return jnp.where(first, a, b), jnp.where(first, b, a)


def hidden_of(part, scale, x):
    tokens, wide = part.shape
    part = part.reshape(4, tokens // 4, wide)
    both = pick(part, x)
    sent = part.astype(bf16)
    for step in (1, 2, 3):
        both = both + shifted(pick(sent, x + step), "rx", step).astype(f32)
    if scale is not None:
        both = both * scale[:, None]
    gate, upward = both[:, : wide // 2], both[:, wide // 2 :]
    return (jax.nn.silu(gate) * upward).astype(bf16)


def down(hidden, w, core):
    mine, other = hidden, other_core(hidden)
    first = core == 0
    both = jnp.concatenate([jnp.where(first, mine, other), jnp.where(first, other, mine)], 0)
    part = jnp.dot(both, w, preferred_element_type=f32).astype(bf16)
    got = exchange(part.reshape(32, 8, w.shape[1]), ("dp", "rz", "cb"))
    summed = jnp.sum(got.reshape(2, 16, 8, w.shape[1]).astype(f32), axis=1)
    return jnp.concatenate([summed[0], summed[1]], axis=1)


def shards(
    tokens,
    first_gain,
    first_gate,
    first_up,
    first_down,
    first_branch,
    second_gain,
    second_gate,
    second_up,
    second_down,
    second_branch,
):
    core = lax.axis_index("dp")
    y = lax.axis_index("cb")
    n_tok, width = tokens.shape
    full = width * 16

    wide = tokens.astype(f32)
    squares = jnp.sum(wide * wide, axis=1)
    scaled = (wide * first_gain.astype(f32)).astype(bf16)
    scaled = jnp.concatenate(halves_by_core(scaled, core), axis=1)

    z = lax.axis_index("rz")
    x = lax.axis_index("rx")
    w1 = up_weights(first_gate, first_up, core, z)
    x1 = [shifted(scaled, "rz", step) if step else scaled for step in range(4)]

    sq = jnp.broadcast_to(squares.reshape(1, 4, 1, 128), (4, 4, 1, 128)).reshape(16, 1, 128)
    mean = jnp.sum(exchange(sq, ("rz", "rx")), axis=(0, 1)) / full
    scale = lax.rsqrt(mean + epsilon)

    rows = tokens.reshape(4, 4, 4, 8, width)
    rows = lax.dynamic_index_in_dim(rows, y, 2, keepdims=False)
    rows = rows.transpose(1, 0, 2, 3).reshape(16, 8, width)
    side = jnp.stack([first_branch, second_gain, second_branch], 0)
    side = jnp.concatenate([side, jnp.zeros((5, width), bf16)], 0)
    side = jnp.concatenate([rows, jnp.broadcast_to(side[None], (16, 8, width))], 1)
    side = exchange(side, ("rz", "rx"))
    side = side.transpose(1, 0, 2).reshape(16, full)
    own = side[:8].astype(f32)
    branch1 = side[8].astype(f32)
    gain2 = side[9].astype(f32)
    branch2 = side[10].astype(f32)

    w2 = down_weights(first_down, core, x)

    half = width // 2
    part = 0.0
    for own_x, own_w in zip(x1, w1):
        part = part + jnp.dot(own_x[:, :half], own_w, preferred_element_type=f32)
        part = part + jnp.dot(own_x[:, half:], other_core(own_w), preferred_element_type=f32)
    hidden = hidden_of(part, scale, x)
    total = down(hidden, w2, core)
    middle = (residual_scale * own + 0.5 * branch1 * total).astype(bf16)

    v1 = up_weights(second_gate, second_up, core, z)
    v2 = down_weights(second_down, core, x)

    mid = middle.astype(f32)
    square = jnp.mean(mid * mid, axis=1, keepdims=True)
    normed = (mid * lax.rsqrt(square + epsilon) * gain2).astype(bf16)
    normed = normed.reshape(8, 4, 4, width)
    mine, other = halves_by_core(normed, core)
    normed = jnp.stack([mine, other], 3)
    normed = normed.transpose(2, 0, 1, 3, 4).reshape(4, 1, 8, full // 4)
    send = jnp.broadcast_to(normed, (4, 16, 8, full // 4)).reshape(64, 8, full // 4)
    x2 = exchange(send, ("rx", "rz", "cb")).reshape(n_tok, full // 4)
    whole = jnp.zeros((4, 2, half, 2 * first_gate.shape[1] // 4), bf16)
    for step, own_w in enumerate(v1):
        piece = jnp.stack([own_w, other_core(own_w)], 0)[None]
        whole = lax.dynamic_update_slice(whole, piece, ((z - step) % 4, 0, 0, 0))
    part = jnp.dot(x2, whole.reshape(full // 4, -1), preferred_element_type=f32)
    hidden = hidden_of(part, None, x)
    total = down(hidden, v2, core)
    out = (residual_scale * mid + 0.5 * branch2 * total).astype(bf16)
    out = out.reshape(8, 4, 4, width).transpose(2, 1, 0, 3)
    send = jnp.broadcast_to(out[:, :, None], (4, 4, 4, 8, width)).reshape(64, 8, width)
    return exchange(send, ("rx", "rz", "cb")).reshape(n_tok, width)


def solution(mesh):
    fine = Mesh(mesh.devices.reshape(4, 4, 4, 2), ("rz", "rx", "cb", "dp"))
    ra = ("rz", "rx")
    vector, up, dn = P(ra), P(ra, "cb"), P(("cb", *ra), None)
    layer = (vector, up, up, dn, vector)
    return jax.shard_map(
        shards,
        mesh=fine,
        in_specs=(P("dp", ra), *layer, *layer),
        out_specs=P("dp", ra),
        check_vma=False,
    )
```

```python
import jax
import jax.numpy as jnp
from jax import lax
from jax.experimental import pallas as pl
from jax.experimental.pallas import tpu as pltpu
from jax.sharding import Mesh, PartitionSpec as P

epsilon = 1e-06
residual_scale = 0.25
f32 = jnp.float32
bf16 = jnp.bfloat16
VMEM = pl.BlockSpec(memory_space=pltpu.VMEM)
SMEM = pl.BlockSpec(memory_space=pltpu.SMEM)
ANY = pl.BlockSpec(memory_space=pl.ANY)
PARAMS = pltpu.CompilerParams(vmem_limit_bytes=40 * 2**20)


def exchange(x, axes):
    return lax.all_to_all(x, axes, 0, 0, tiled=True)


def other_core(x):
    return lax.ppermute(x, "dp", [(0, 1), (1, 0)])


def shifted(x, axis, step):
    return lax.ppermute(x, axis, [(i, (i + step) % 4) for i in range(4)])


def dot(a, b, dims):
    return lax.dot_general(a, b, (dims, ((), ())), preferred_element_type=f32)


def silu(v):
    return v / (1.0 + jnp.exp(-v))


def tiles(v, core):
    lead, width = v.shape[:-1], v.shape[-1]
    split = v.reshape(*lead, width // 256, 2, 128)
    mine, other = split[..., 0, :], split[..., 1, :]
    first = core == 0
    mine, other = jnp.where(first, mine, other), jnp.where(first, other, mine)
    return jnp.concatenate([mine.reshape(*lead, -1), other.reshape(*lead, -1)], -1)


def own_tiles(v, core):
    rows, width = v.shape
    split = v.reshape(rows, width // 256, 2, 128)
    return jnp.where(core == 0, split[:, :, 0], split[:, :, 1]).reshape(rows, width // 2)


def up_part(place, *refs):
    xs, mine, other, own, sends, acc = refs[:4], refs[4:8], refs[8:12], refs[12], refs[13:16], refs[16]
    total = None
    for x, a, b in zip(xs, mine, other):
        part = dot(x[...], jnp.concatenate([a[...], b[...]], 0), ((1,), (0,)))
        total = part if total is None else total + part
    acc[...] = total
    x = place[0]
    own[...] = acc[pl.ds(x * 128, 128), :]
    for step, send in enumerate(sends, 1):
        send[...] = acc[pl.ds(((x + step) % 4) * 128, 128), :].astype(bf16)


def down_part(place, own, a, b, c, scale, *refs):
    w_mine, w_other, out, whole, sems = refs[:4], refs[4:8], refs[8], refs[9], refs[10]
    half = whole.shape[1] // 2
    rows = whole.shape[0] // 4
    x = place[0]
    copies = []
    for step in range(4):
        at = pl.ds(((x + 4 - step) % 4) * rows, rows)
        for side, w in enumerate((w_mine, w_other)):
            to = whole.at[at, pl.ds(side * half, half)]
            copies.append(pltpu.make_async_copy(w[step], to, sems.at[2 * step + side]))
    for copy in copies:
        copy.start()
    both = own[...] + a[...].astype(f32) + b[...].astype(f32) + c[...].astype(f32)
    both = both * scale[...]
    part = both.shape[1] // 2
    hidden = (silu(both[:, :part]) * both[:, part:]).astype(bf16)
    for copy in copies:
        copy.wait()
    out[...] = dot(hidden, whole[...], ((1,), (0,))).astype(bf16)


def join(got, tokens, branch, gain, send):
    total = jnp.sum(got[...].astype(f32), axis=0)
    middle = (residual_scale * tokens[...].astype(f32) + 0.5 * branch[...] * total).astype(bf16)
    mid = middle.astype(f32)
    square = jnp.mean(mid * mid, axis=1, keepdims=True)
    normed = (mid * lax.rsqrt(square + epsilon) * gain[...]).astype(bf16)
    full = normed.shape[1]
    for x in range(4):
        for z in range(4):
            block = (4 * z + x) * 128
            send[4 * x + z, :, :full] = normed
            send[4 * x + z, :, full : full + 128] = middle[:, block : block + 128]
            send[4 * x + z, :, full + 128 :] = middle[:, full // 2 + block : full // 2 + block + 128]


def feed_forward(x, *refs):
    ups, downs, out = refs[:8], refs[8:16], refs[16]
    up, whole, up_sems, down_sems = refs[17:]
    blocks, cols, _ = ups[0].shape
    rows, half = downs[0].shape
    groups = up_sems.shape[0]
    each = blocks // groups
    up_copies, down_copies = [], []
    for group in range(groups):
        at = pl.ds(group * each, each)
        copies = []
        for step in range(4):
            for side in range(2):
                to = up.at[side, at, pl.ds(step * cols, cols), :]
                source = ups[2 * step + side].at[at]
                copies.append(pltpu.make_async_copy(source, to, up_sems.at[group, 2 * step + side]))
        up_copies.append(copies)
    for step in range(4):
        for side in range(2):
            to = whole.at[pl.ds(step * rows, rows), pl.ds(side * half, half)]
            down_copies.append(pltpu.make_async_copy(downs[2 * step + side], to, down_sems.at[2 * step + side]))
    for copy in [c for copies in up_copies for c in copies] + down_copies:
        copy.start()
    total = None
    for group in range(groups):
        for copy in up_copies[group]:
            copy.wait()
        for block in range(group * each, (group + 1) * each):
            lanes = slice(block * 128, block * 128 + 128)
            others = slice(half + block * 128, half + block * 128 + 128)
            tokens = jnp.concatenate([x[:, lanes], x[:, others]], 1)
            weights = jnp.concatenate([up[0, block], up[1, block]], 1)
            part = dot(weights, tokens, ((1,), (1,)))
            total = part if total is None else total + part
    hidden = []
    for step in range(4):
        gate = total[step * cols : step * cols + cols // 2]
        upward = total[step * cols + cols // 2 : (step + 1) * cols]
        hidden.append(silu(gate) * upward)
    hidden = jnp.concatenate(hidden, 0).T.astype(bf16)
    for copy in down_copies:
        copy.wait()
    for part in range(4):
        wide = half // 4
        mine = dot(hidden, whole[:, part * wide : (part + 1) * wide], ((1,), (0,))).astype(bf16)
        other = dot(hidden, whole[:, half + part * wide : half + (part + 1) * wide], ((1,), (0,))).astype(bf16)
        for i in range(wide // 128):
            out[part * (wide // 128) + i, :, :128] = mine[:, i * 128 : (i + 1) * 128]
            out[part * (wide // 128) + i, :, 128:] = other[:, i * 128 : (i + 1) * 128]


def shards(
    tokens,
    first_gain,
    first_gate,
    first_up,
    first_down,
    first_branch,
    second_gain,
    second_gate,
    second_up,
    second_down,
    second_branch,
):
    core, x, y, z = (lax.axis_index(name) for name in ("dp", "rx", "cb", "rz"))
    place = x.reshape(1).astype(jnp.int32)
    n_tok, width = tokens.shape
    full = width * 16
    half = width // 2
    cols = first_gate.shape[1]
    part = cols // 4

    wide = tokens.astype(f32)
    squares = jnp.sum(wide * wide, axis=1)
    scaled = tiles((wide * first_gain.astype(f32)).astype(bf16), core)

    def up_piece(step, row_half):
        to = (z + step) % 4
        pieces = [lax.dynamic_slice(w, (row_half * half, to * part), (half, part)) for w in (first_gate, first_up)]
        return jnp.concatenate(pieces, 1)

    w1 = [up_piece(0, core)] + [shifted(up_piece(step, core), "rz", step) for step in (1, 2, 3)]
    x1 = [scaled] + [shifted(scaled, "rz", step) for step in (1, 2, 3)]
    w1_other = [up_piece(0, 1 - core)] + [other_core(w) for w in w1[1:]]

    rows = tokens.reshape(4, 4, 4, 8, width)
    rows = lax.dynamic_index_in_dim(rows, y, 2, keepdims=False)
    rows = rows.transpose(1, 0, 2, 3).reshape(16, 8, width)
    high = lax.reduce_precision(squares, 8, 7)
    mid = lax.reduce_precision(squares - high, 8, 7)
    low = squares - high - mid
    pieces = [v.astype(bf16).reshape(4, 1, 128) for v in (high, mid, low)]
    sq = jnp.concatenate(
        [jnp.concatenate(pieces[:2], 2), jnp.concatenate([pieces[2], jnp.zeros((4, 1, 128), bf16)], 2)], 1
    )
    sq = jnp.broadcast_to(sq[None], (4, 4, 2, width)).reshape(16, 2, width)
    side = jnp.stack([first_branch, second_gain], 0)
    side = jnp.broadcast_to(side[None], (16, 2, width))
    side = jnp.concatenate([rows, side, sq, jnp.zeros((16, 4, width), bf16)], 1)
    side = exchange(side, ("rz", "rx"))
    sq = jnp.sum(side[:, 10:12].astype(f32), axis=0)
    sq = sq[0, :half] + sq[0, half:] + sq[1, :half]
    scale = lax.rsqrt(sq / full + epsilon)[:, None]
    side = tiles(side.transpose(1, 0, 2).reshape(16, full), core)

    w2 = own_tiles(first_down, core)
    w2 = [w2] + [shifted(w2, "rx", step) for step in (1, 2, 3)]
    w2_other = [other_core(w) for w in w2]

    def turned(w):
        mine = lax.dynamic_slice_in_dim(w, core * half, half, 0)
        return mine.T.reshape(16, cols // 16, half)

    v1 = exchange(jnp.concatenate([turned(second_gate), turned(second_up)], 1), ("rz", "rx"))
    v1 = [v1] + [shifted(v1, "cb", step) for step in (1, 2, 3)]
    v2 = own_tiles(second_down, core)
    v2 = [v2] + [shifted(v2, "cb", step) for step in (1, 2, 3)]
    v1 = [w for mine in v1 for w in (mine, other_core(mine))]
    v2 = [w for mine in v2 for w in (mine, other_core(mine))]

    own, *sends = pl.pallas_call(
        up_part,
        out_shape=[jax.ShapeDtypeStruct((n_tok // 4, 2 * part), t) for t in (f32, bf16, bf16, bf16)],
        in_specs=[SMEM] + [VMEM] * 12,
        out_specs=[VMEM] * 4,
        scratch_shapes=[pltpu.VMEM((n_tok, 2 * part), f32)],
        compiler_params=PARAMS,
        name="up_part",
    )(place, *x1, *w1, *w1_other)
    got = [shifted(send, "rx", step) for step, send in enumerate(sends, 1)]
    partial = pl.pallas_call(
        down_part,
        out_shape=jax.ShapeDtypeStruct((n_tok // 4, full), bf16),
        in_specs=[SMEM] + [VMEM] * 5 + [ANY] * 8,
        out_specs=VMEM,
        scratch_shapes=[pltpu.VMEM((part, full), bf16), pltpu.SemaphoreType.DMA((8,))],
        compiler_params=PARAMS,
        name="down_part",
    )(place, own, *got, scale, *w2, *w2_other)
    got = exchange(partial.reshape(16, 8, full), ("rz", "cb"))
    send = pl.pallas_call(
        join,
        out_shape=jax.ShapeDtypeStruct((16, 8, full + width), bf16),
        in_specs=[VMEM] * 4,
        out_specs=VMEM,
        compiler_params=PARAMS,
        name="join",
    )(got, side[:8], side[8:9].astype(f32), side[9:10].astype(f32))
    got = exchange(send, ("rx", "rz"))
    x2 = got[:, :, :full].reshape(n_tok // 4, full)
    middle = got[:, :, full:].reshape(n_tok // 4, width).astype(f32)
    partial = pl.pallas_call(
        feed_forward,
        out_shape=jax.ShapeDtypeStruct((16, n_tok // 4, width), bf16),
        in_specs=[VMEM] + [ANY] * 16,
        out_specs=VMEM,
        scratch_shapes=[
            pltpu.VMEM((2, 16, 2 * part, half), bf16),
            pltpu.VMEM((part, full), bf16),
            pltpu.SemaphoreType.DMA((4, 8)),
            pltpu.SemaphoreType.DMA((8,)),
        ],
        compiler_params=PARAMS,
        name="feed_forward",
    )(x2, *v1, *v2)
    total = jnp.sum(exchange(partial, ("rz", "rx")).astype(f32), axis=0)
    branch = tiles(second_branch.astype(f32), core)
    out = (residual_scale * middle + 0.5 * branch * total).astype(bf16)
    a, b = out[:, :half], out[:, half:]
    out = jnp.concatenate([jnp.where(core == 0, a, b), jnp.where(core == 0, b, a)], 1)
    parts = [out] + [shifted(out, "cb", step) for step in (1, 2, 3)]
    blocks = []
    for at in range(4):
        back = (y - at) % 4
        block = jnp.where(back == 0, parts[0], jnp.where(back == 1, parts[1], jnp.where(back == 2, parts[2], parts[3])))
        blocks.append(block.reshape(16, 8, width))
    return jnp.stack(blocks, 1).reshape(n_tok, width)


def solution(mesh):
    fine = Mesh(mesh.devices.reshape(4, 4, 4, 2), ("rz", "rx", "cb", "dp"))
    ra = ("rz", "rx")
    vector, up, dn = P(ra), P(ra, "cb"), P(("cb", *ra), None)
    layer = (vector, up, up, dn, vector)
    return jax.shard_map(
        shards,
        mesh=fine,
        in_specs=(P("dp", ra), *layer, *layer),
        out_specs=P("dp", ra),
        check_vma=False,
    )
```

```python
import jax
import jax.numpy as jnp
from jax import lax
from jax.experimental import pallas as pl
from jax.experimental.pallas import tpu as pltpu
from jax.sharding import Mesh, PartitionSpec as P

epsilon = 1e-06
residual_scale = 0.25
f32 = jnp.float32
bf16 = jnp.bfloat16
VMEM = pl.BlockSpec(memory_space=pltpu.VMEM)
SMEM = pl.BlockSpec(memory_space=pltpu.SMEM)
ANY = pl.BlockSpec(memory_space=pl.ANY)


def exchange(x, axes):
    return lax.all_to_all(x, axes, 0, 0, tiled=True)


def other_core(x):
    return lax.ppermute(x, "dp", [(0, 1), (1, 0)])


def shifted(x, axis, step):
    return lax.ppermute(x, axis, [(i, (i + step) % 4) for i in range(4)])


def dot(a, b, dims):
    return lax.dot_general(a, b, (dims, ((), ())), preferred_element_type=f32)


def silu(v):
    return v / (1.0 + jnp.exp(-v))


def at_lane(core, half):
    return pl.ds(pl.multiple_of(core * half, 128), half)


def pack(core_ref, z_ref, gate, upward, down1, down2, *refs):
    sends, mine1, mine2, sems = refs[:3], refs[3], refs[4], refs[5]
    core, z = core_ref[0], z_ref[0]
    rows, wide = sends[0].shape
    part, half = wide // 2, mine1.shape[1]
    copies = []
    for step, send in enumerate(sends, 1):
        at = pl.ds(pl.multiple_of(((z + step) % 4) * part, 128), part)
        for side, w in enumerate((gate, upward)):
            source = w.at[pl.ds(core * rows, rows), at]
            copies.append((source, send.at[:, pl.ds(side * part, part)]))
    for w, mine in ((down1, mine1), (down2, mine2)):
        copies.append((w.at[:, at_lane(core, half)], mine))
    copies = [pltpu.make_async_copy(*c, sems.at[i]) for i, c in enumerate(copies)]
    for copy in copies:
        copy.start()
    for copy in copies:
        copy.wait()


def up_part(core_ref, x_ref, z_ref, gate, upward, *refs):
    xs, mine, other = refs[:4], refs[4:7], refs[7:10]
    own, sends, acc, whole, sems = refs[10], refs[11:14], refs[14], refs[15], refs[16]
    core, x, z = core_ref[0], x_ref[0], z_ref[0]
    rows, wide = mine[0].shape
    part = wide // 2
    at = pl.ds(pl.multiple_of(z * part, 128), part)
    copies = [[]]
    for side, w in enumerate((gate, upward)):
        copies[0].append((w.at[:, at], whole.at[0, :, pl.ds(side * part, part)]))
    for step in range(3):
        here = (mine[step], whole.at[step + 1, pl.ds(core * rows, rows), :])
        there = (other[step], whole.at[step + 1, pl.ds((1 - core) * rows, rows), :])
        copies.append([here, there])
    copies = [
        [pltpu.make_async_copy(*c, sems.at[2 * step + i]) for i, c in enumerate(group)]
        for step, group in enumerate(copies)
    ]
    for group in copies:
        for copy in group:
            copy.start()
    total = None
    for step, tokens in enumerate(xs):
        for copy in copies[step]:
            copy.wait()
        one = dot(tokens[...], whole[step], ((1,), (0,)))
        total = one if total is None else total + one
    acc[...] = total
    own[...] = acc[pl.ds(x * 128, 128), :]
    for step, send in enumerate(sends, 1):
        send[...] = acc[pl.ds(((x + step) % 4) * 128, 128), :].astype(bf16)


def down_part(core_ref, x_ref, own, a, b, c, scale, w, *refs):
    mine, other, out, whole, sems = refs[:3], refs[3:6], refs[6], refs[7], refs[8]
    core, x = core_ref[0], x_ref[0]
    rows, full = w.shape
    half = full // 2
    copies = [(w, whole.at[pl.ds(x * rows, rows), :])]
    for step in range(1, 4):
        at = pl.ds(((x + 4 - step) % 4) * rows, rows)
        copies.append((mine[step - 1], whole.at[at, at_lane(core, half)]))
        copies.append((other[step - 1], whole.at[at, at_lane(1 - core, half)]))
    copies = [pltpu.make_async_copy(*c, sems.at[i]) for i, c in enumerate(copies)]
    for copy in copies:
        copy.start()
    both = own[...] + a[...].astype(f32) + b[...].astype(f32) + c[...].astype(f32)
    both = both * scale[...]
    part = both.shape[1] // 2
    hidden = (silu(both[:, :part]) * both[:, part:]).astype(bf16)
    for copy in copies:
        copy.wait()
    out[...] = dot(hidden, whole[...], ((1,), (0,))).astype(bf16)


def join(got, side, branch, gain, send):
    total = jnp.sum(got[...].astype(f32), axis=0)
    middle = (residual_scale * side[...].astype(f32) + 0.5 * branch[...] * total).astype(bf16)
    mid = middle.astype(f32)
    square = jnp.mean(mid * mid, axis=1, keepdims=True)
    normed = (mid * lax.rsqrt(square + epsilon) * gain[...]).astype(bf16)
    full = normed.shape[1]
    width = full // 16
    for x in range(4):
        for z in range(4):
            block = (4 * z + x) * width
            send[4 * x + z, :, :full] = normed
            send[4 * x + z, :, full:] = middle[:, block : block + width]


def feed_forward(core_ref, got, w_down, *refs):
    ups, mine, other, out = refs[:8], refs[8:11], refs[11:14], refs[14]
    tokens, up, whole, up_sems, down_sems = refs[15:]
    core = core_ref[0]
    blocks, cols, width = ups[0].shape
    rows, full = w_down.shape
    half = full // 2
    groups = up_sems.shape[0]
    each = blocks // groups
    up_copies = []
    for group in range(groups):
        at = pl.ds(group * each, each)
        copies = []
        for step in range(4):
            for side, place in enumerate((core, 1 - core)):
                to = up.at[at, pl.ds(step * 2 * cols + place * cols, cols), :]
                source = ups[2 * step + side].at[at]
                copies.append(pltpu.make_async_copy(source, to, up_sems.at[group, 2 * step + side]))
        up_copies.append(copies)
    down_copies = [(w_down, whole.at[pl.ds(0, rows), :])]
    for step in range(1, 4):
        at = pl.ds(step * rows, rows)
        down_copies.append((mine[step - 1], whole.at[at, at_lane(core, half)]))
        down_copies.append((other[step - 1], whole.at[at, at_lane(1 - core, half)]))
    down_copies = [pltpu.make_async_copy(*c, down_sems.at[i]) for i, c in enumerate(down_copies)]
    for copy in [c for copies in up_copies for c in copies] + down_copies:
        copy.start()
    for j in range(got.shape[0]):
        tokens[8 * j : 8 * j + 8, :] = got[j, :, :full]
    total = None
    for group in range(groups):
        for copy in up_copies[group]:
            copy.wait()
        for block in range(group * each, (group + 1) * each):
            part = dot(up[block], tokens[:, block * width : (block + 1) * width], ((1,), (1,)))
            total = part if total is None else total + part
    hidden = []
    for step in range(4):
        gate = total[2 * step * cols : (2 * step + 1) * cols]
        upward = total[(2 * step + 1) * cols : (2 * step + 2) * cols]
        hidden.append(silu(gate) * upward)
    hidden = jnp.concatenate(hidden, 0).T.astype(bf16)
    for copy in down_copies:
        copy.wait()
    for block in range(blocks):
        lanes = slice(block * width, (block + 1) * width)
        out[block] = dot(hidden, whole[:, lanes], ((1,), (0,))).astype(bf16)


def shards(
    tokens,
    first_gain,
    first_gate,
    first_up,
    first_down,
    first_branch,
    second_gain,
    second_gate,
    second_up,
    second_down,
    second_branch,
):
    core, x, y, z = (lax.axis_index(name) for name in ("dp", "rx", "cb", "rz"))
    core_ref, x_ref, z_ref = (i.astype(jnp.int32).reshape(1) for i in (core, x, z))
    n_tok, width = tokens.shape
    full = width * 16
    half = width // 2
    cols = first_gate.shape[1]
    part = cols // 4
    few = n_tok // 4
    w_half = jax.ShapeDtypeStruct((first_down.shape[0], full // 2), bf16)

    def kernel(body, ins, *outs, scratch=(), mib=16):
        flat = list(outs)
        return pl.pallas_call(
            body,
            out_shape=flat if len(flat) > 1 else flat[0],
            in_specs=ins,
            out_specs=[VMEM] * len(flat) if len(flat) > 1 else VMEM,
            scratch_shapes=list(scratch),
            compiler_params=pltpu.CompilerParams(vmem_limit_bytes=mib * 2**20),
        )

    *w1, d1, d2 = kernel(
        pack,
        [SMEM] * 2 + [ANY] * 4,
        *[jax.ShapeDtypeStruct((half, 2 * part), bf16)] * 3,
        w_half,
        w_half,
        scratch=[pltpu.SemaphoreType.DMA((8,))],
    )(core_ref, z_ref, first_gate, first_up, first_down, second_down)
    wide = tokens.astype(f32)
    squares = jnp.sum(wide * wide, axis=1)
    scaled = (wide * first_gain.astype(f32)).astype(bf16)

    w1 = [shifted(w, "rz", step) for step, w in enumerate(w1, 1)]
    x1 = [scaled] + [shifted(scaled, "rz", step) for step in (1, 2, 3)]
    w1_other = [other_core(w) for w in w1]

    rows = tokens.reshape(4, 4, 4, 8, width)
    rows = lax.dynamic_index_in_dim(rows, y, 2, keepdims=False)
    rows = rows.transpose(1, 0, 2, 3).reshape(16, 8, width)
    high = lax.reduce_precision(squares, 8, 7)
    mid = lax.reduce_precision(squares - high, 8, 7)
    low = squares - high - mid
    pieces = [v.astype(bf16).reshape(4, 1, 128) for v in (high, mid, low)]
    sq = jnp.concatenate(
        [jnp.concatenate(pieces[:2], 2), jnp.concatenate([pieces[2], jnp.zeros((4, 1, 128), bf16)], 2)], 1
    )
    sq = jnp.broadcast_to(sq[None], (4, 4, 2, width)).reshape(16, 2, width)
    side = jnp.stack([first_branch, second_gain], 0)
    side = jnp.broadcast_to(side[None], (16, 2, width))
    turned = jnp.where(core == 0, second_gate, second_up).T.reshape(16, cols // 16, width)
    side = jnp.concatenate([turned, rows, side, sq, jnp.zeros((16, 4, width), bf16)], 1)
    side = exchange(side, ("rz", "rx"))
    v1 = side[:, : cols // 16]
    side = side[:, cols // 16 :]
    sq = jnp.sum(side[:, 10:12].astype(f32), axis=0)
    sq = sq[0, :half] + sq[0, half:] + sq[1, :half]
    scale = lax.rsqrt(sq / full + epsilon)[:, None]
    side = side.transpose(1, 0, 2).reshape(16, full)
    rows, branch, gain = side[:8], side[8:9].astype(f32), side[9:10].astype(f32)

    d1 = [shifted(d1, "rx", step) for step in (1, 2, 3)]
    d2 = [shifted(d2, "cb", step) for step in (1, 2, 3)]
    v1 = [v1] + [shifted(v1, "cb", step) for step in (1, 2, 3)]
    d1_other = [other_core(w) for w in d1]
    d2_other = [other_core(w) for w in d2]
    v1 = [w for mine in v1 for w in (mine, other_core(mine))]

    own, *sends = kernel(
        up_part,
        [SMEM] * 3 + [ANY] * 2 + [VMEM] * 4 + [ANY] * 6,
        jax.ShapeDtypeStruct((few, 2 * part), f32),
        *[jax.ShapeDtypeStruct((few, 2 * part), bf16)] * 3,
        scratch=[
            pltpu.VMEM((n_tok, 2 * part), f32),
            pltpu.VMEM((4, width, 2 * part), bf16),
            pltpu.SemaphoreType.DMA((8,)),
        ],
    )(core_ref, x_ref, z_ref, first_gate, first_up, *x1, *w1, *w1_other)
    got = [shifted(send, "rx", step) for step, send in enumerate(sends, 1)]
    partial = kernel(
        down_part,
        [SMEM] * 2 + [VMEM] * 5 + [ANY] * 7,
        jax.ShapeDtypeStruct((few, full), bf16),
        scratch=[pltpu.VMEM((part, full), bf16), pltpu.SemaphoreType.DMA((7,))],
    )(core_ref, x_ref, own, *got, scale, first_down, *d1, *d1_other)
    got = exchange(partial.reshape(16, 8, full), ("rz", "cb"))
    send = kernel(
        join,
        [VMEM] * 4,
        jax.ShapeDtypeStruct((16, 8, full + width), bf16),
    )(got, rows, branch, gain)
    got = exchange(send, ("rx", "rz"))
    middle = got[:, :, full:].reshape(few, width).astype(f32)
    partial = kernel(
        feed_forward,
        [SMEM, VMEM] + [ANY] * 15,
        jax.ShapeDtypeStruct((16, few, width), bf16),
        scratch=[
            pltpu.VMEM((few, full), bf16),
            pltpu.VMEM((16, 2 * part, width), bf16),
            pltpu.VMEM((part, full), bf16),
            pltpu.SemaphoreType.DMA((4, 8)),
            pltpu.SemaphoreType.DMA((7,)),
        ],
        mib=24,
    )(core_ref, got, second_down, *v1, *d2, *d2_other)
    got = exchange(partial, ("rz", "rx"))
    total = jnp.sum(got.astype(f32), axis=0)
    out = (residual_scale * middle + 0.5 * second_branch.astype(f32) * total).astype(bf16)
    parts = [out] + [shifted(out, "cb", step) for step in (1, 2, 3)]
    blocks = []
    for at in range(4):
        back = (y - at) % 4
        block = jnp.where(back == 0, parts[0], jnp.where(back == 1, parts[1], jnp.where(back == 2, parts[2], parts[3])))
        blocks.append(block.reshape(16, 8, width))
    return jnp.stack(blocks, 1).reshape(n_tok, width)


def solution(mesh):
    fine = Mesh(mesh.devices.reshape(4, 4, 4, 2), ("rz", "rx", "cb", "dp"))
    ra = ("rz", "rx")
    vector, up, dn = P(ra), P(ra, "cb"), P(("cb", *ra), None)
    layer = (vector, up, up, dn, vector)
    return jax.shard_map(
        shards,
        mesh=fine,
        in_specs=(P("dp", ra), *layer, *layer),
        out_specs=P("dp", ra),
        check_vma=False,
    )
```

```python
import jax
import jax.numpy as jnp
from jax import lax
from jax.experimental import pallas as pl
from jax.experimental.pallas import tpu as pltpu
from jax.sharding import Mesh, PartitionSpec as P

epsilon = 1e-06
residual_scale = 0.25
f32 = jnp.float32
bf16 = jnp.bfloat16
VMEM = pl.BlockSpec(memory_space=pltpu.VMEM)
SMEM = pl.BlockSpec(memory_space=pltpu.SMEM)
HBM = pl.BlockSpec(memory_space=pltpu.HBM)


def exchange(x, axes):
    return lax.all_to_all(x, axes, 0, 0, tiled=True)


def other_core(x):
    return lax.ppermute(x, "dp", [(0, 1), (1, 0)])


def shifted(x, axis, step):
    return lax.ppermute(x, axis, [(i, (i + step) % 4) for i in range(4)])


def dot(a, b, dims):
    return lax.dot_general(a, b, (dims, ((), ())), preferred_element_type=f32)


def silu(v):
    return v / (1.0 + jnp.exp(-v))


def at_lane(core, half):
    return pl.ds(pl.multiple_of(core * half, 128), half)


def together(pairs, sems):
    copies = [pltpu.make_async_copy(*pair, sems.at[i]) for i, pair in enumerate(pairs)]
    for copy in copies:
        copy.start()
    return copies


def wait_for(copies):
    for copy in copies:
        copy.wait()


def pack(core_ref, z_ref, gain, tokens, gate, upward, down1, down2, *refs):
    sends, mine1, mine2, scaled, here, sems = refs[:3], refs[3], refs[4], refs[5], refs[6], refs[7]
    core, z = core_ref[0], z_ref[0]
    rows, wide = sends[0].shape
    part, half = wide // 2, mine1.shape[1]
    pairs = [(tokens, here)]
    for step, send in enumerate(sends, 1):
        at = pl.ds(pl.multiple_of(((z + step) % 4) * part, 128), part)
        for side, w in enumerate((gate, upward)):
            source = w.at[pl.ds(core * rows, rows), at]
            pairs.append((source, send.at[:, pl.ds(side * part, part)]))
    for w, mine in ((down1, mine1), (down2, mine2)):
        pairs.append((w.at[:, at_lane(core, half)], mine))
    copies = together(pairs, sems)
    copies[0].wait()
    scaled[...] = (here[...].astype(f32) * gain[...].astype(f32)).astype(bf16)
    wait_for(copies[1:])


def message(core_ref, y_ref, branch, gain, here, tokens, gate, upward, out, picked, sems):
    core, y = core_ref[0], y_ref[0]
    width, cols = picked.shape
    each = cols // 16

    @pl.when(core == 0)
    def _():
        pltpu.make_async_copy(gate, picked, sems.at[16]).start()

    @pl.when(core == 1)
    def _():
        pltpu.make_async_copy(upward, picked, sems.at[16]).start()

    pairs = []
    for z in range(4):
        for x in range(4):
            source = tokens.at[pl.ds(x * 128 + 32 * z + 8 * y, 8), :]
            pairs.append((source, out.at[4 * z + x, pl.ds(each, 8), :]))
    copies = together(pairs, sems)
    wide = here[...].astype(f32)
    squares = lax.dot_general(
        jnp.ones((8, width), f32),
        wide * wide,
        (((1,), (1,)), ((), ())),
        precision=lax.Precision.HIGHEST,
        preferred_element_type=f32,
    )
    high = squares.astype(bf16).astype(f32)
    mid = (squares - high).astype(bf16).astype(f32)
    low = squares - high - mid
    row = lax.broadcasted_iota(jnp.int32, (8, width), 0)
    fixed = jnp.where(row == 0, branch[...].astype(f32), jnp.where(row == 1, gain[...].astype(f32), 0.0))
    blocks = []
    for x in range(4):
        at = slice(128 * x, 128 * x + 128)
        first = jnp.concatenate([high[:, at], mid[:, at]], 1)
        second = jnp.concatenate([low[:, at], jnp.zeros_like(low[:, at])], 1)
        blocks.append(jnp.where(row == 2, first, jnp.where(row == 3, second, fixed)).astype(bf16))
    pltpu.make_async_copy(gate, picked, sems.at[16]).wait()
    turned = picked[...].T
    for z in range(4):
        for x in range(4):
            to = 4 * z + x
            out[to, :each, :] = turned[to * each : (to + 1) * each, :]
            out[to, each + 8 :, :] = blocks[x]
    wait_for(copies)


def up_part(core_ref, x_ref, z_ref, first_x, gate, upward, *refs):
    xs, mine, other = refs[:3], refs[3:6], refs[6:9]
    own, sends, acc, whole, held, sems = refs[9], refs[10:13], refs[13], refs[14], refs[15], refs[16]
    core, x, z = core_ref[0], x_ref[0], z_ref[0]
    rows, wide = mine[0].shape
    part = wide // 2
    at = pl.ds(pl.multiple_of(z * part, 128), part)
    copies = [[]]
    for side, w in enumerate((gate, upward)):
        copies[0].append((w.at[:, at], whole.at[0, :, pl.ds(side * part, part)]))
    for step in range(3):
        here = (mine[step], whole.at[step + 1, pl.ds(core * rows, rows), :])
        there = (other[step], whole.at[step + 1, pl.ds((1 - core) * rows, rows), :])
        copies.append([here, there, (xs[step], held.at[step])])
    copies = [together(group, sems.at[step]) for step, group in enumerate(copies)]
    total = None
    for step in range(4):
        wait_for(copies[step])
        tokens = held[step - 1] if step else first_x[...]
        one = dot(tokens, whole[step], ((1,), (0,)))
        total = one if total is None else total + one
    acc[...] = total
    own[...] = acc[pl.ds(x * 128, 128), :]
    for step, send in enumerate(sends, 1):
        send[...] = acc[pl.ds(((x + step) % 4) * 128, 128), :].astype(bf16)


def down_part(core_ref, x_ref, own, a, b, c, side, w, *refs):
    mine, other, out, whole, small, sems = refs[:3], refs[3:6], refs[6], refs[7], refs[8], refs[9]
    core, x = core_ref[0], x_ref[0]
    rows, full = w.shape
    half = full // 2
    copies = [(side.at[:, pl.ds(rows, 16), :], small), (w, whole.at[pl.ds(x * rows, rows), :])]
    for step in range(1, 4):
        at = pl.ds(((x + 4 - step) % 4) * rows, rows)
        copies.append((mine[step - 1], whole.at[at, at_lane(core, half)]))
        copies.append((other[step - 1], whole.at[at, at_lane(1 - core, half)]))
    copies = together(copies, sems)
    both = own[...] + a[...].astype(f32) + b[...].astype(f32) + c[...].astype(f32)
    copies[0].wait()
    squares = jnp.sum(small[...].astype(f32), axis=0)[10:12]
    squares = squares[0:1, :128] + squares[0:1, 128:] + squares[1:2, :128]
    scale = lax.rsqrt(squares / full + epsilon)
    both = both * jnp.broadcast_to(scale, (8, 128)).T[:, :1]
    part = both.shape[1] // 2
    hidden = (silu(both[:, :part]) * both[:, part:]).astype(bf16)
    wait_for(copies[1:])
    out[...] = dot(hidden, whole[...], ((1,), (0,))).astype(bf16)


def join(got, side, send, small, sem):
    copy = pltpu.make_async_copy(side.at[:, pl.ds(side.shape[1] - 16, 16), :], small, sem)
    copy.start()
    total = jnp.sum(got[...].astype(f32), axis=0)
    copy.wait()
    blocks = [small[i].astype(f32) for i in range(16)]
    tokens, branch, gain = (jnp.concatenate([b[at] for b in blocks], 1) for at in (slice(0, 8), slice(8, 9), slice(9, 10)))
    middle = (residual_scale * tokens + 0.5 * branch * total).astype(bf16)
    mid = middle.astype(f32)
    square = jnp.mean(mid * mid, axis=1, keepdims=True)
    normed = (mid * lax.rsqrt(square + epsilon) * gain).astype(bf16)
    full = normed.shape[1]
    width = full // 16
    for x in range(4):
        for z in range(4):
            block = (4 * z + x) * width
            send[4 * x + z, :, :full] = normed
            send[4 * x + z, :, full:] = middle[:, block : block + width]


def finish(got, branch, send, out, middle, sems):
    count, rows = send.shape[:2]
    width = out.shape[1]
    pairs = [(send.at[:, :, pl.ds(send.shape[2] - width, width)], middle)]
    copies = together(pairs, sems)
    total = jnp.sum(got[...].astype(f32), axis=0)
    wait_for(copies)
    for j in range(count):
        at = slice(j * rows, (j + 1) * rows)
        mid = middle[j].astype(f32)
        out[at, :] = (residual_scale * mid + 0.5 * branch[...].astype(f32) * total[at]).astype(bf16)


def feed_forward(core_ref, got, w_down, *refs):
    ups, mine, other, out = refs[:8], refs[8:11], refs[11:14], refs[14]
    tokens, up, whole, up_sems, down_sems = refs[15:]
    core = core_ref[0]
    blocks, cols, width = ups[0].shape
    rows, full = w_down.shape
    half = full // 2
    groups = up_sems.shape[0]
    each = blocks // groups
    up_copies = []
    for group in range(groups):
        at = pl.ds(group * each, each)
        copies = []
        for step in range(4):
            for side, place in enumerate((core, 1 - core)):
                to = up.at[at, pl.ds(step * 2 * cols + place * cols, cols), :]
                source = ups[2 * step + side].at[at]
                copies.append(pltpu.make_async_copy(source, to, up_sems.at[group, 2 * step + side]))
        up_copies.append(copies)
    down_copies = [(w_down, whole.at[pl.ds(0, rows), :])]
    for step in range(1, 4):
        at = pl.ds(step * rows, rows)
        down_copies.append((mine[step - 1], whole.at[at, at_lane(core, half)]))
        down_copies.append((other[step - 1], whole.at[at, at_lane(1 - core, half)]))
    down_copies = [pltpu.make_async_copy(*c, down_sems.at[i]) for i, c in enumerate(down_copies)]
    for copy in [c for copies in up_copies for c in copies] + down_copies:
        copy.start()
    for j in range(got.shape[0]):
        tokens[8 * j : 8 * j + 8, :] = got[j, :, :full]
    total = None
    for group in range(groups):
        for copy in up_copies[group]:
            copy.wait()
        for block in range(group * each, (group + 1) * each):
            part = dot(up[block], tokens[:, block * width : (block + 1) * width], ((1,), (1,)))
            total = part if total is None else total + part
    hidden = []
    for step in range(4):
        gate = total[2 * step * cols : (2 * step + 1) * cols]
        upward = total[(2 * step + 1) * cols : (2 * step + 2) * cols]
        hidden.append(silu(gate) * upward)
    hidden = jnp.concatenate(hidden, 0).T.astype(bf16)
    for copy in down_copies:
        copy.wait()
    for block in range(blocks):
        lanes = slice(block * width, (block + 1) * width)
        out[block] = dot(hidden, whole[:, lanes], ((1,), (0,))).astype(bf16)


def shards(
    tokens,
    first_gain,
    first_gate,
    first_up,
    first_down,
    first_branch,
    second_gain,
    second_gate,
    second_up,
    second_down,
    second_branch,
):
    core, x, y, z = (lax.axis_index(name) for name in ("dp", "rx", "cb", "rz"))
    core_ref, x_ref, y_ref, z_ref = (i.astype(jnp.int32).reshape(1) for i in (core, x, y, z))
    n_tok, width = tokens.shape
    full = width * 16
    half = width // 2
    cols = first_gate.shape[1]
    part = cols // 4
    few = n_tok // 4
    w_half = jax.ShapeDtypeStruct((first_down.shape[0], full // 2), bf16)

    def kernel(body, ins, *outs, scratch=(), mib=16):
        call = pl.pallas_call(
            body,
            out_shape=list(outs) if len(outs) > 1 else outs[0],
            in_specs=ins,
            out_specs=[VMEM] * len(outs) if len(outs) > 1 else VMEM,
            scratch_shapes=list(scratch),
            compiler_params=pltpu.CompilerParams(vmem_limit_bytes=mib * 2**20),
        )

        def run(*args):
            kept = [pltpu.with_memory_space_constraint(a, pltpu.HBM) if spec is HBM else a for a, spec in zip(args, ins)]
            return call(*kept)

        return run

    dma = pltpu.SemaphoreType.DMA

    *w1, d1, d2, scaled = kernel(
        pack,
        [SMEM] * 2 + [VMEM] + [HBM] * 5,
        *[jax.ShapeDtypeStruct((half, 2 * part), bf16)] * 3,
        w_half,
        w_half,
        jax.ShapeDtypeStruct(tokens.shape, bf16),
        scratch=[pltpu.VMEM(tokens.shape, bf16), dma((9,))],
    )(core_ref, z_ref, first_gain[None], tokens, first_gate, first_up, first_down, second_down)
    w1 = [shifted(w, "rz", step) for step, w in enumerate(w1, 1)]
    x1 = [scaled] + [shifted(scaled, "rz", step) for step in (1, 2, 3)]
    w1_other = [other_core(w) for w in w1]

    side = kernel(
        message,
        [SMEM] * 2 + [VMEM] * 3 + [HBM] * 3,
        jax.ShapeDtypeStruct((16, cols // 16 + 16, width), bf16),
        scratch=[pltpu.VMEM((width, cols), bf16), dma((17,))],
    )(core_ref, y_ref, first_branch[None], second_gain[None], tokens, tokens, second_gate, second_up)
    side = exchange(side, ("rz", "rx"))
    v1 = side[:, : cols // 16]

    d1 = [shifted(d1, "rx", step) for step in (1, 2, 3)]
    d2 = [shifted(d2, "cb", step) for step in (1, 2, 3)]
    v1 = [v1] + [shifted(v1, "cb", step) for step in (1, 2, 3)]
    d1_other = [other_core(w) for w in d1]
    d2_other = [other_core(w) for w in d2]
    v1 = [w for mine in v1 for w in (mine, other_core(mine))]

    own, *sends = kernel(
        up_part,
        [SMEM] * 3 + [VMEM] + [HBM] * 11,
        jax.ShapeDtypeStruct((few, 2 * part), f32),
        *[jax.ShapeDtypeStruct((few, 2 * part), bf16)] * 3,
        scratch=[
            pltpu.VMEM((n_tok, 2 * part), f32),
            pltpu.VMEM((4, width, 2 * part), bf16),
            pltpu.VMEM((3, n_tok, width), bf16),
            dma((4, 3)),
        ],
    )(core_ref, x_ref, z_ref, x1[0], first_gate, first_up, *x1[1:], *w1, *w1_other)
    got = [shifted(send, "rx", step) for step, send in enumerate(sends, 1)]
    partial = kernel(
        down_part,
        [SMEM] * 2 + [VMEM] * 4 + [HBM] * 8,
        jax.ShapeDtypeStruct((few, full), bf16),
        scratch=[pltpu.VMEM((part, full), bf16), pltpu.VMEM((16, 16, width), bf16), dma((8,))],
    )(core_ref, x_ref, own, *got, side, first_down, *d1, *d1_other)
    got = exchange(partial.reshape(16, 8, full), ("rz", "cb"))
    send = kernel(
        join,
        [VMEM, HBM],
        jax.ShapeDtypeStruct((16, 8, full + width), bf16),
        scratch=[pltpu.VMEM((16, 16, width), bf16), dma(())],
    )(got, side)
    rows = exchange(send, ("rx", "rz"))
    partial = kernel(
        feed_forward,
        [SMEM, VMEM] + [HBM] * 15,
        jax.ShapeDtypeStruct((16, few, width), bf16),
        scratch=[
            pltpu.VMEM((few, full), bf16),
            pltpu.VMEM((16, 2 * part, width), bf16),
            pltpu.VMEM((part, full), bf16),
            dma((4, 8)),
            dma((7,)),
        ],
        mib=24,
    )(core_ref, rows, second_down, *v1, *d2, *d2_other)
    partial, branch = lax.optimization_barrier((partial, second_branch[None]))
    got = exchange(partial, ("rz", "rx"))
    out = kernel(
        finish,
        [VMEM, VMEM, HBM],
        jax.ShapeDtypeStruct((few, width), bf16),
        scratch=[pltpu.VMEM((16, 8, width), bf16), dma((1,))],
    )(got, branch, rows)
    parts = [out] + [shifted(out, "cb", step) for step in (1, 2, 3)]
    blocks = []
    for at in range(4):
        back = (y - at) % 4
        block = jnp.where(back == 0, parts[0], jnp.where(back == 1, parts[1], jnp.where(back == 2, parts[2], parts[3])))
        blocks.append(block.reshape(16, 8, width))
    return jnp.stack(blocks, 1).reshape(n_tok, width)


def solution(mesh):
    fine = Mesh(mesh.devices.reshape(4, 4, 4, 2), ("rz", "rx", "cb", "dp"))
    ra = ("rz", "rx")
    vector, up, dn = P(ra), P(ra, "cb"), P(("cb", *ra), None)
    layer = (vector, up, up, dn, vector)
    return jax.shard_map(
        shards,
        mesh=fine,
        in_specs=(P("dp", ra), *layer, *layer),
        out_specs=P("dp", ra),
        check_vma=False,
    )
```

```python
import jax
import jax.numpy as jnp
from jax import lax
from jax.experimental import pallas as pl
from jax.experimental.pallas import tpu as pltpu
from jax.sharding import Mesh, PartitionSpec as P

epsilon = 1e-06
residual_scale = 0.25
f32 = jnp.float32
bf16 = jnp.bfloat16
VMEM = pl.BlockSpec(memory_space=pltpu.VMEM)
SMEM = pl.BlockSpec(memory_space=pltpu.SMEM)
HBM = pl.BlockSpec(memory_space=pltpu.HBM)


def exchange(x, axes):
    return lax.all_to_all(x, axes, 0, 0, tiled=True)


def other_core(x):
    return lax.ppermute(x, "dp", [(0, 1), (1, 0)])


def shifted(x, axis, step):
    return lax.ppermute(x, axis, [(i, (i + step) % 4) for i in range(4)])


def dot(a, b, dims):
    return lax.dot_general(a, b, (dims, ((), ())), preferred_element_type=f32)


def silu(v):
    return v / (1.0 + jnp.exp(-v))


def at_lane(core, half):
    return pl.ds(pl.multiple_of(core * half, 128), half)


def together(pairs, sems):
    copies = [pltpu.make_async_copy(*pair, sems.at[i]) for i, pair in enumerate(pairs)]
    for copy in copies:
        copy.start()
    return copies


def wait_for(copies):
    for copy in copies:
        copy.wait()


def pack(core_ref, z_ref, gain, tokens, gate, upward, down1, down2, *refs):
    sends, mine1, mine2, scaled, here, sems = refs[:3], refs[3], refs[4], refs[5], refs[6], refs[7]
    core, z = core_ref[0], z_ref[0]
    rows, wide = sends[0].shape
    part, half = wide // 2, mine1.shape[1]
    pairs = [(tokens, here)]
    for step, send in enumerate(sends, 1):
        at = pl.ds(pl.multiple_of(((z + step) % 4) * part, 128), part)
        for side, w in enumerate((gate, upward)):
            source = w.at[pl.ds(core * rows, rows), at]
            pairs.append((source, send.at[:, pl.ds(side * part, part)]))
    for w, mine in ((down1, mine1), (down2, mine2)):
        pairs.append((w.at[:, at_lane(core, half)], mine))
    copies = together(pairs, sems)
    copies[0].wait()
    scaled[...] = (here[...].astype(f32) * gain[...].astype(f32)).astype(bf16)
    wait_for(copies[1:])


def message(core_ref, y_ref, branch, gain, here, tokens, gate, upward, out, picked, sems):
    core, y = core_ref[0], y_ref[0]
    width, cols = picked.shape
    each = cols // 16

    @pl.when(core == 0)
    def _():
        pltpu.make_async_copy(gate, picked, sems.at[16]).start()

    @pl.when(core == 1)
    def _():
        pltpu.make_async_copy(upward, picked, sems.at[16]).start()

    pairs = []
    for z in range(4):
        for x in range(4):
            source = tokens.at[pl.ds(128 * y + 32 * x + 8 * z, 8), :]
            pairs.append((source, out.at[4 * z + x, pl.ds(each, 8), :]))
    copies = together(pairs, sems)
    wide = jnp.concatenate([here[128 * j + 32 * x : 128 * j + 32 * x + 32, :] for x in range(4) for j in range(4)], 0)
    wide = wide.astype(f32)
    wide = wide * wide
    turned = (wide[:, :128] + wide[:, 128:]).T
    squares = jnp.broadcast_to(jnp.sum(turned, axis=0, keepdims=True), (8, turned.shape[1]))
    high = squares.astype(bf16).astype(f32)
    mid = (squares - high).astype(bf16).astype(f32)
    low = squares - high - mid
    row = lax.broadcasted_iota(jnp.int32, (8, width), 0)
    fixed = jnp.where(row == 0, branch[...].astype(f32), jnp.where(row == 1, gain[...].astype(f32), 0.0))
    blocks = []
    for x in range(4):
        at = slice(128 * x, 128 * x + 128)
        first = jnp.concatenate([high[:, at], mid[:, at]], 1)
        second = jnp.concatenate([low[:, at], jnp.zeros_like(low[:, at])], 1)
        blocks.append(jnp.where(row == 2, first, jnp.where(row == 3, second, fixed)).astype(bf16))
    pltpu.make_async_copy(gate, picked, sems.at[16]).wait()
    turned = picked[...].T
    for z in range(4):
        for x in range(4):
            to = 4 * z + x
            out[to, :each, :] = turned[to * each : (to + 1) * each, :]
            out[to, each + 8 :, :] = blocks[x]
    wait_for(copies)


def up_part(core_ref, x_ref, z_ref, first_x, gate, upward, *refs):
    xs, mine, other = refs[:3], refs[3:6], refs[6:9]
    own, sends, acc, whole, held, sems = refs[9], refs[10:13], refs[13], refs[14], refs[15], refs[16]
    core, x, z = core_ref[0], x_ref[0], z_ref[0]
    rows, wide = mine[0].shape
    part = wide // 2
    at = pl.ds(pl.multiple_of(z * part, 128), part)
    copies = [[]]
    for side, w in enumerate((gate, upward)):
        copies[0].append((w.at[:, at], whole.at[0, :, pl.ds(side * part, part)]))
    for step in range(3):
        here = (mine[step], whole.at[step + 1, pl.ds(core * rows, rows), :])
        there = (other[step], whole.at[step + 1, pl.ds((1 - core) * rows, rows), :])
        copies.append([here, there, (xs[step], held.at[step])])
    copies = [together(group, sems.at[step]) for step, group in enumerate(copies)]
    total = None
    for step in range(4):
        wait_for(copies[step])
        tokens = held[step - 1] if step else first_x[...]
        one = dot(tokens, whole[step], ((1,), (0,)))
        total = one if total is None else total + one
    acc[...] = total
    for j in range(4):
        at = slice(32 * j, 32 * j + 32)
        own[at, :] = acc[pl.ds(128 * j + 32 * x, 32), :]
        for step, send in enumerate(sends, 1):
            send[at, :] = acc[pl.ds(128 * j + 32 * ((x + step) % 4), 32), :].astype(bf16)


def down_part(core_ref, x_ref, own, a, b, c, side, w, *refs):
    mine, other, out, whole, small, sems = refs[:3], refs[3:6], refs[6], refs[7], refs[8], refs[9]
    core, x = core_ref[0], x_ref[0]
    rows, full = w.shape
    half = full // 2
    copies = [(side.at[:, pl.ds(rows, 16), :], small), (w, whole.at[pl.ds(x * rows, rows), :])]
    for step in range(1, 4):
        at = pl.ds(((x + 4 - step) % 4) * rows, rows)
        copies.append((mine[step - 1], whole.at[at, at_lane(core, half)]))
        copies.append((other[step - 1], whole.at[at, at_lane(1 - core, half)]))
    copies = together(copies, sems)
    both = own[...] + a[...].astype(f32) + b[...].astype(f32) + c[...].astype(f32)
    copies[0].wait()
    squares = jnp.sum(small[...].astype(f32), axis=0)[10:12]
    squares = squares[0:1, :128] + squares[0:1, 128:] + squares[1:2, :128]
    scale = lax.rsqrt(squares / full + epsilon)
    both = both * jnp.broadcast_to(scale, (8, 128)).T[:, :1]
    part = both.shape[1] // 2
    hidden = (silu(both[:, :part]) * both[:, part:]).astype(bf16)
    wait_for(copies[1:])
    out[...] = dot(hidden, whole[...], ((1,), (0,))).astype(bf16)


def join(got, side, send, small, sem):
    copy = pltpu.make_async_copy(side.at[:, pl.ds(side.shape[1] - 16, 16), :], small, sem)
    copy.start()
    total = jnp.sum(got[...].astype(f32), axis=0)
    copy.wait()
    blocks = [small[i].astype(f32) for i in range(16)]
    tokens, branch, gain = (jnp.concatenate([b[at] for b in blocks], 1) for at in (slice(0, 8), slice(8, 9), slice(9, 10)))
    middle = (residual_scale * tokens + 0.5 * branch * total).astype(bf16)
    mid = middle.astype(f32)
    square = jnp.mean(mid * mid, axis=1, keepdims=True)
    normed = (mid * lax.rsqrt(square + epsilon) * gain).astype(bf16)
    full = normed.shape[1]
    width = full // 16
    for x in range(4):
        for z in range(4):
            block = (4 * z + x) * width
            send[4 * x + z, :, :full] = normed
            send[4 * x + z, :, full:] = middle[:, block : block + width]


def finish(got, branch, send, out, middle, sems):
    count, rows = send.shape[:2]
    width = out.shape[2]
    pairs = [(send.at[:, :, pl.ds(send.shape[2] - width, width)], middle)]
    copies = together(pairs, sems)
    total = jnp.sum(got[...].astype(f32), axis=0)
    wait_for(copies)
    for j in range(count):
        at = slice(j * rows, (j + 1) * rows)
        mid = middle[j].astype(f32)
        value = (residual_scale * mid + 0.5 * branch[...].astype(f32) * total[at]).astype(bf16)
        for y in range(4):
            out[y, at, :] = value


def gated(core, tokens, ups, up, sems):
    blocks, cols, width = ups[0].shape
    groups = sems.shape[0]
    each = blocks // groups
    pending = []
    for group in range(groups):
        at = pl.ds(group * each, each)
        pairs = []
        for i, source in enumerate(ups):
            place = core if i % 2 == 0 else 1 - core
            to = up.at[at, pl.ds((i // 2) * 2 * cols + place * cols, cols), :]
            pairs.append((source.at[at], to))
        pending.append(together(pairs, sems.at[group]))

    def finish():
        total = None
        for group in range(groups):
            wait_for(pending[group])
            for block in range(group * each, (group + 1) * each):
                part = dot(up[block], tokens[:, block * width : (block + 1) * width], ((1,), (1,)))
                total = part if total is None else total + part
        hidden = []
        for i in range(len(ups) // 2):
            gate = total[2 * i * cols : (2 * i + 1) * cols]
            hidden.append(silu(gate) * total[(2 * i + 1) * cols : (2 * i + 2) * cols])
        return jnp.concatenate(hidden, 0)

    return finish


def ff_near(core_ref, got, *refs):
    ups, out, tokens, up, sems = refs[:6], refs[6], refs[7], refs[8], refs[9]
    finish = gated(core_ref[0], tokens, ups, up, sems)
    for j in range(got.shape[0]):
        tokens[8 * j : 8 * j + 8, :] = got[j, :, : tokens.shape[1]]
    out[...] = finish()


def ff_far(core_ref, got, near, w_down, *refs):
    ups, mine, other, out = refs[:2], refs[2:5], refs[5:8], refs[8]
    tokens, up, whole, up_sems, down_sems = refs[9:]
    core = core_ref[0]
    rows, full = w_down.shape
    half = full // 2
    finish = gated(core, tokens, ups, up, up_sems)
    pairs = [(w_down, whole.at[pl.ds(0, rows), :])]
    for i, piece in enumerate((0, 2, 1), 1):
        at = pl.ds(i * rows, rows)
        pairs.append((mine[piece], whole.at[at, at_lane(core, half)]))
        pairs.append((other[piece], whole.at[at, at_lane(1 - core, half)]))
    copies = together(pairs, down_sems)
    for j in range(got.shape[0]):
        tokens[8 * j : 8 * j + 8, :] = got[j, :, :full]
    hidden = jnp.concatenate([near[...], finish()], 0).T.astype(bf16)
    wait_for(copies)
    width = out.shape[2]
    for z in range(4):
        for x in range(4):
            lanes = slice((4 * z + x) * width, (4 * z + x + 1) * width)
            out[4 * x + z] = dot(hidden, whole[:, lanes], ((1,), (0,))).astype(bf16)


def shards(
    tokens,
    first_gain,
    first_gate,
    first_up,
    first_down,
    first_branch,
    second_gain,
    second_gate,
    second_up,
    second_down,
    second_branch,
):
    core, x, y, z = (lax.axis_index(name) for name in ("dp", "rx", "cb", "rz"))
    core_ref, x_ref, y_ref, z_ref = (i.astype(jnp.int32).reshape(1) for i in (core, x, y, z))
    n_tok, width = tokens.shape
    full = width * 16
    half = width // 2
    cols = first_gate.shape[1]
    part = cols // 4
    few = n_tok // 4
    w_half = jax.ShapeDtypeStruct((first_down.shape[0], full // 2), bf16)

    def kernel(body, ins, *outs, scratch=(), mib=16):
        call = pl.pallas_call(
            body,
            out_shape=list(outs) if len(outs) > 1 else outs[0],
            in_specs=ins,
            out_specs=[VMEM] * len(outs) if len(outs) > 1 else VMEM,
            scratch_shapes=list(scratch),
            compiler_params=pltpu.CompilerParams(vmem_limit_bytes=mib * 2**20),
        )

        def run(*args):
            kept = [pltpu.with_memory_space_constraint(a, pltpu.HBM) if spec is HBM else a for a, spec in zip(args, ins)]
            return call(*kept)

        return run

    dma = pltpu.SemaphoreType.DMA

    *w1, d1, d2, scaled = kernel(
        pack,
        [SMEM] * 2 + [VMEM] + [HBM] * 5,
        *[jax.ShapeDtypeStruct((half, 2 * part), bf16)] * 3,
        w_half,
        w_half,
        jax.ShapeDtypeStruct(tokens.shape, bf16),
        scratch=[pltpu.VMEM(tokens.shape, bf16), dma((9,))],
    )(core_ref, z_ref, first_gain[None], tokens, first_gate, first_up, first_down, second_down)
    w1 = [shifted(w, "rz", step) for step, w in enumerate(w1, 1)]
    x1 = [scaled] + [shifted(scaled, "rz", step) for step in (1, 2, 3)]
    w1_other = [other_core(w) for w in w1]

    side = kernel(
        message,
        [SMEM] * 2 + [VMEM] * 3 + [HBM] * 3,
        jax.ShapeDtypeStruct((16, cols // 16 + 16, width), bf16),
        scratch=[pltpu.VMEM((width, cols), bf16), dma((17,))],
    )(core_ref, y_ref, first_branch[None], second_gain[None], tokens, tokens, second_gate, second_up)
    side = exchange(side, ("rz", "rx"))
    v1 = side[:, : cols // 16]

    d1 = [shifted(d1, "rx", step) for step in (1, 2, 3)]
    d2 = [shifted(d2, "cb", step) for step in (1, 2, 3)]
    near = [shifted(v1, "cb", step) for step in (1, 3)]
    v1 = [v1, near[0], shifted(v1, "cb", 2), near[1]]
    d1_other = [other_core(w) for w in d1]
    d2_other = [other_core(w) for w in d2]
    near = [w for mine in (v1[0], v1[1], v1[3]) for w in (mine, other_core(mine))]
    far = [v1[2], other_core(v1[2])]

    own, *sends = kernel(
        up_part,
        [SMEM] * 3 + [VMEM] + [HBM] * 11,
        jax.ShapeDtypeStruct((few, 2 * part), f32),
        *[jax.ShapeDtypeStruct((few, 2 * part), bf16)] * 3,
        scratch=[
            pltpu.VMEM((n_tok, 2 * part), f32),
            pltpu.VMEM((4, width, 2 * part), bf16),
            pltpu.VMEM((3, n_tok, width), bf16),
            dma((4, 3)),
        ],
    )(core_ref, x_ref, z_ref, x1[0], first_gate, first_up, *x1[1:], *w1, *w1_other)
    got = [shifted(send, "rx", step) for step, send in enumerate(sends, 1)]
    partial = kernel(
        down_part,
        [SMEM] * 2 + [VMEM] * 4 + [HBM] * 8,
        pltpu.VMEM((few, full), bf16),
        scratch=[pltpu.VMEM((part, full), bf16), pltpu.VMEM((16, 16, width), bf16), dma((8,))],
    )(core_ref, x_ref, own, *got, side, first_down, *d1, *d1_other)
    got = exchange(partial.reshape(16, 8, full), ("cb", "rz"))
    send = kernel(
        join,
        [VMEM, HBM],
        jax.ShapeDtypeStruct((16, 8, full + width), bf16),
        scratch=[pltpu.VMEM((16, 16, width), bf16), dma(())],
    )(got, side)
    rows = exchange(send, ("rx", "rz"))
    hidden = kernel(
        ff_near,
        [SMEM, VMEM] + [HBM] * 6,
        jax.ShapeDtypeStruct((3 * part // 4, few), f32),
        scratch=[pltpu.VMEM((few, full), bf16), pltpu.VMEM((16, 6 * part // 4, width), bf16), dma((4, 6))],
    )(core_ref, rows, *near)
    partial = kernel(
        ff_far,
        [SMEM, VMEM, VMEM] + [HBM] * 9,
        pltpu.VMEM((16, few, width), bf16),
        scratch=[
            pltpu.VMEM((few, full), bf16),
            pltpu.VMEM((16, part // 2, width), bf16),
            pltpu.VMEM((part, full), bf16),
            dma((2, 2)),
            dma((7,)),
        ],
    )(core_ref, rows, hidden, second_down, *far, *d2, *d2_other)
    partial, branch = lax.optimization_barrier((partial, second_branch[None]))
    got = exchange(partial, ("rx", "rz"))
    out = kernel(
        finish,
        [VMEM, VMEM, HBM],
        pltpu.VMEM((4, few, width), bf16),
        scratch=[pltpu.VMEM((16, 8, width), bf16), dma((1,))],
    )(got, branch, rows)
    out = exchange(out, "cb")
    return out.reshape(n_tok, width)


def solution(mesh):
    fine = Mesh(mesh.devices.reshape(4, 4, 4, 2), ("rz", "rx", "cb", "dp"))
    ra = ("rz", "rx")
    vector, up, dn = P(ra), P(ra, "cb"), P(("cb", *ra), None)
    layer = (vector, up, up, dn, vector)
    return jax.shard_map(
        shards,
        mesh=fine,
        in_specs=(P("dp", ra), *layer, *layer),
        out_specs=P("dp", ra),
        check_vma=False,
    )
```

```python
import jax
import jax.numpy as jnp
from jax import lax
from jax.experimental import pallas as pl
from jax.experimental.pallas import tpu as pltpu
from jax.sharding import Mesh, PartitionSpec as P

epsilon = 1e-06
residual_scale = 0.25
f32 = jnp.float32
bf16 = jnp.bfloat16
VMEM = pl.BlockSpec(memory_space=pltpu.VMEM)
SMEM = pl.BlockSpec(memory_space=pltpu.SMEM)
HBM = pl.BlockSpec(memory_space=pltpu.HBM)


def exchange(x, axes):
    return lax.all_to_all(x, axes, 0, 0, tiled=True)


def other_core(x):
    return lax.ppermute(x, "dp", [(0, 1), (1, 0)])


def shifted(x, axis, step):
    return lax.ppermute(x, axis, [(i, (i + step) % 4) for i in range(4)])


def dot(a, b, dims):
    return lax.dot_general(a, b, (dims, ((), ())), preferred_element_type=f32)


def silu(v):
    return v / (1.0 + jnp.exp(-v))


def at_lane(core, half):
    return pl.ds(pl.multiple_of(core * half, 128), half)


def together(pairs, sems):
    copies = [pltpu.make_async_copy(*pair, sems.at[i]) for i, pair in enumerate(pairs)]
    for copy in copies:
        copy.start()
    return copies


def wait_for(copies):
    for copy in copies:
        copy.wait()


def pack(core_ref, z_ref, gain, tokens, gate, upward, down1, down2, *refs):
    sends, mine1, mine2, scaled, here, sems = refs[:3], refs[3], refs[4], refs[5], refs[6], refs[7]
    core, z = core_ref[0], z_ref[0]
    rows, wide = sends[0].shape
    part, half = wide // 2, mine1.shape[1]
    pairs = [(tokens, here)]
    for step, send in enumerate(sends, 1):
        at = pl.ds(pl.multiple_of(((z + step) % 4) * part, 128), part)
        for side, w in enumerate((gate, upward)):
            source = w.at[pl.ds(core * rows, rows), at]
            pairs.append((source, send.at[:, pl.ds(side * part, part)]))
    for w, mine in ((down1, mine1), (down2, mine2)):
        pairs.append((w.at[:, at_lane(core, half)], mine))
    copies = together(pairs, sems)
    copies[0].wait()
    scaled[...] = (here[...].astype(f32) * gain[...].astype(f32)).astype(bf16)
    wait_for(copies[1:])


def token_rows(x):
    return [128 * j + 32 * x + 8 * z for z in range(4) for j in range(4)]


def message(core_ref, y_ref, branch, gain, here, tokens, gate, upward, out, picked, sems):
    core, y = core_ref[0], y_ref[0]
    width, cols = picked.shape
    each = cols // 16

    @pl.when(core == 0)
    def _():
        pltpu.make_async_copy(gate, picked, sems.at[16]).start()

    @pl.when(core == 1)
    def _():
        pltpu.make_async_copy(upward, picked, sems.at[16]).start()

    pairs = []
    for z in range(4):
        for x in range(4):
            source = tokens.at[pl.ds(128 * y + 32 * x + 8 * z, 8), :]
            pairs.append((source, out.at[4 * z + x, pl.ds(each, 8), :]))
    copies = together(pairs, sems)
    wide = here[...].astype(f32)
    wide = jnp.concatenate([wide[at : at + 8] for x in range(4) for at in token_rows(x)], 0)
    wide = wide * wide
    turned = (wide[:, :128] + wide[:, 128:]).T
    squares = jnp.broadcast_to(jnp.sum(turned, axis=0, keepdims=True), (8, turned.shape[1]))
    high = squares.astype(bf16).astype(f32)
    mid = (squares - high).astype(bf16).astype(f32)
    low = squares - high - mid
    row = lax.broadcasted_iota(jnp.int32, (8, width), 0)
    fixed = jnp.where(row == 0, branch[...].astype(f32), jnp.where(row == 1, gain[...].astype(f32), 0.0))
    blocks = []
    for x in range(4):
        at = slice(128 * x, 128 * x + 128)
        first = jnp.concatenate([high[:, at], mid[:, at]], 1)
        second = jnp.concatenate([low[:, at], jnp.zeros_like(low[:, at])], 1)
        blocks.append(jnp.where(row == 2, first, jnp.where(row == 3, second, fixed)).astype(bf16))
    pltpu.make_async_copy(gate, picked, sems.at[16]).wait()
    turned = picked[...].T
    for z in range(4):
        for x in range(4):
            to = 4 * z + x
            out[to, :each, :] = turned[to * each : (to + 1) * each, :]
            out[to, each + 8 :, :] = blocks[x]
    wait_for(copies)


def up_part(core_ref, x_ref, z_ref, first_x, gate, upward, *refs):
    xs, mine, other = refs[:3], refs[3:6], refs[6:9]
    own, sends, acc, whole, held, sems = refs[9], refs[10:13], refs[13], refs[14], refs[15], refs[16]
    core, x, z = core_ref[0], x_ref[0], z_ref[0]
    rows, wide = mine[0].shape
    part = wide // 2
    at = pl.ds(pl.multiple_of(z * part, 128), part)
    copies = [[]]
    for side, w in enumerate((gate, upward)):
        copies[0].append((w.at[:, at], whole.at[0, :, pl.ds(side * part, part)]))
    for step in range(3):
        here = (mine[step], whole.at[step + 1, pl.ds(core * rows, rows), :])
        there = (other[step], whole.at[step + 1, pl.ds((1 - core) * rows, rows), :])
        copies.append([here, there, (xs[step], held.at[step])])
    copies = [together(group, sems.at[step]) for step, group in enumerate(copies)]
    total = None
    for step in range(4):
        wait_for(copies[step])
        tokens = held[step - 1] if step else first_x[...]
        one = dot(tokens, whole[step], ((1,), (0,)))
        total = one if total is None else total + one
    acc[...] = total

    def block(to):
        return jnp.concatenate([acc[pl.ds(at, 8), :] for at in token_rows(to)], 0)

    own[...] = block(x)
    for step, send in enumerate(sends, 1):
        send[...] = block((x + step) % 4).astype(bf16)


def down_part(core_ref, x_ref, own, a, b, c, side, w, *refs):
    mine, other, out, whole, small, sems = refs[:3], refs[3:6], refs[6], refs[7], refs[8], refs[9]
    core, x = core_ref[0], x_ref[0]
    rows, full = w.shape
    half = full // 2
    copies = [(side.at[:, pl.ds(rows, 16), :], small), (w, whole.at[pl.ds(x * rows, rows), :])]
    for step in range(1, 4):
        at = pl.ds(((x + 4 - step) % 4) * rows, rows)
        copies.append((mine[step - 1], whole.at[at, at_lane(core, half)]))
        copies.append((other[step - 1], whole.at[at, at_lane(1 - core, half)]))
    copies = together(copies, sems)
    both = own[...] + a[...].astype(f32) + b[...].astype(f32) + c[...].astype(f32)
    copies[0].wait()
    squares = jnp.sum(small[...].astype(f32), axis=0)[10:12]
    squares = squares[0:1, :128] + squares[0:1, 128:] + squares[1:2, :128]
    scale = lax.rsqrt(squares / full + epsilon)
    both = both * jnp.broadcast_to(scale, (8, 128)).T[:, :1]
    part = both.shape[1] // 2
    hidden = (silu(both[:, :part]) * both[:, part:]).astype(bf16)
    wait_for(copies[1:])
    out[...] = dot(hidden, whole[...], ((1,), (0,))).astype(bf16)


def join(got, side, send, small, sem):
    copy = pltpu.make_async_copy(side.at[:, pl.ds(side.shape[1] - 16, 16), :], small, sem)
    copy.start()
    total = jnp.sum(got[...].astype(f32), axis=0)
    copy.wait()
    blocks = [small[i].astype(f32) for i in range(16)]
    tokens, branch, gain = (jnp.concatenate([b[at] for b in blocks], 1) for at in (slice(0, 8), slice(8, 9), slice(9, 10)))
    middle = (residual_scale * tokens + 0.5 * branch * total).astype(bf16)
    mid = middle.astype(f32)
    square = jnp.mean(mid * mid, axis=1, keepdims=True)
    normed = (mid * lax.rsqrt(square + epsilon) * gain).astype(bf16)
    full = normed.shape[1]
    width = full // 16
    for x in range(4):
        for z in range(4):
            block = (4 * z + x) * width
            send[4 * x + z, :, :full] = normed
            send[4 * x + z, :, full:] = middle[:, block : block + width]


def finish(got, branch, send, out, middle, sems):
    count, rows = send.shape[:2]
    width = out.shape[2]
    pairs = [(send.at[:, :, pl.ds(send.shape[2] - width, width)], middle)]
    copies = together(pairs, sems)
    total = jnp.sum(got[...].astype(f32), axis=0)
    wait_for(copies)
    for j in range(count):
        at = slice(j * rows, (j + 1) * rows)
        mid = middle[j].astype(f32)
        value = (residual_scale * mid + 0.5 * branch[...].astype(f32) * total[at]).astype(bf16)
        for y in range(4):
            out[y, at, :] = value


def gated(core, tokens, sources, up, sems):
    blocks, rows, width = up.shape
    cols = 96
    groups = sems.shape[0]
    each = blocks // groups
    pending = []
    for group in range(groups):
        pairs = []
        for w, first, slot, side in sources:
            begin = group * each - first
            if 0 <= begin < w.shape[0]:
                place = 1 - core if side else core
                to = up.at[pl.ds(group * each, each), pl.ds(slot * 2 * cols + place * cols, cols), :]
                pairs.append((w.at[pl.ds(begin, each), pl.ds(0, cols), :], to))
        pending.append(together(pairs, sems.at[group]))

    def finish():
        total = None
        for group in range(groups):
            wait_for(pending[group])
            for block in range(group * each, (group + 1) * each):
                part = dot(up[block], tokens[:, block * width : (block + 1) * width], ((1,), (1,)))
                total = part if total is None else total + part
        hidden = []
        for i in range(rows // (2 * cols)):
            gate = total[2 * i * cols : (2 * i + 1) * cols]
            hidden.append(silu(gate) * total[(2 * i + 1) * cols : (2 * i + 2) * cols])
        return jnp.concatenate(hidden, 0)

    return finish


def ff_near(core_ref, got, *refs):
    ups, out, tokens, up, sems = refs[:10], refs[10], refs[11], refs[12], refs[13]
    half = up.shape[0] // 2
    sources = [(ups[0], 0, 0, 0), (ups[1], 0, 0, 1)]
    for i, w in enumerate(ups[2:]):
        sources.append((w, half * (i // 2 % 2), 1 + i // 4, i % 2))
    finish = gated(core_ref[0], tokens, sources, up, sems)
    for j in range(got.shape[0]):
        tokens[8 * j : 8 * j + 8, :] = got[j, :, : tokens.shape[1]]
    out[...] = finish()


def ff_far(core_ref, got, near, w_down, *refs):
    ups, mine, other, out = refs[:4], refs[4:7], refs[7:10], refs[10]
    tokens, up, whole, up_sems, down_sems = refs[11:]
    core = core_ref[0]
    rows, full = w_down.shape
    half = full // 2
    sources = [(w, up.shape[0] // 2 * (i // 2), 0, i % 2) for i, w in enumerate(ups)]
    finish = gated(core, tokens, sources, up, up_sems)
    pairs = [(w_down, whole.at[pl.ds(0, rows), :])]
    for i, piece in enumerate((0, 2, 1), 1):
        at = pl.ds(i * rows, rows)
        pairs.append((mine[piece], whole.at[at, at_lane(core, half)]))
        pairs.append((other[piece], whole.at[at, at_lane(1 - core, half)]))
    copies = together(pairs, down_sems)
    for j in range(got.shape[0]):
        tokens[8 * j : 8 * j + 8, :] = got[j, :, :full]
    hidden = jnp.concatenate([near[...], finish()], 0).T.astype(bf16)
    wait_for(copies)
    width = out.shape[2]
    for z in range(4):
        for x in range(4):
            lanes = slice((4 * z + x) * width, (4 * z + x + 1) * width)
            out[4 * x + z] = dot(hidden, whole[:, lanes], ((1,), (0,))).astype(bf16)


def shards(
    tokens,
    first_gain,
    first_gate,
    first_up,
    first_down,
    first_branch,
    second_gain,
    second_gate,
    second_up,
    second_down,
    second_branch,
):
    core, x, y, z = (lax.axis_index(name) for name in ("dp", "rx", "cb", "rz"))
    core_ref, x_ref, y_ref, z_ref = (i.astype(jnp.int32).reshape(1) for i in (core, x, y, z))
    n_tok, width = tokens.shape
    full = width * 16
    half = width // 2
    cols = first_gate.shape[1]
    part = cols // 4
    few = n_tok // 4
    w_half = jax.ShapeDtypeStruct((first_down.shape[0], full // 2), bf16)

    def kernel(body, ins, *outs, scratch=(), mib=16):
        call = pl.pallas_call(
            body,
            out_shape=list(outs) if len(outs) > 1 else outs[0],
            in_specs=ins,
            out_specs=[VMEM] * len(outs) if len(outs) > 1 else VMEM,
            scratch_shapes=list(scratch),
            compiler_params=pltpu.CompilerParams(vmem_limit_bytes=mib * 2**20),
        )

        def run(*args):
            kept = [pltpu.with_memory_space_constraint(a, pltpu.HBM) if spec is HBM else a for a, spec in zip(args, ins)]
            return call(*kept)

        return run

    dma = pltpu.SemaphoreType.DMA

    *w1, d1, d2, scaled = kernel(
        pack,
        [SMEM] * 2 + [VMEM] + [HBM] * 5,
        *[jax.ShapeDtypeStruct((half, 2 * part), bf16)] * 3,
        w_half,
        w_half,
        jax.ShapeDtypeStruct(tokens.shape, bf16),
        scratch=[pltpu.VMEM(tokens.shape, bf16), dma((9,))],
    )(core_ref, z_ref, first_gain[None], tokens, first_gate, first_up, first_down, second_down)
    w1 = [shifted(w, "rz", step) for step, w in enumerate(w1, 1)]
    x1 = [scaled] + [shifted(scaled, "rz", step) for step in (1, 2, 3)]
    w1_other = [other_core(w) for w in w1]

    side = kernel(
        message,
        [SMEM] * 2 + [VMEM] * 3 + [HBM] * 3,
        jax.ShapeDtypeStruct((16, cols // 16 + 16, width), bf16),
        scratch=[pltpu.VMEM((width, cols), bf16), dma((17,))],
    )(core_ref, y_ref, first_branch[None], second_gain[None], tokens, tokens, second_gate, second_up)
    side = exchange(side, ("rz", "rx"))

    def ring(w, axis):
        back, ahead = shifted(w, axis, 1), shifted(w, axis, 3)
        return [back, shifted(back, axis, 1), ahead]

    def swapped(ws):
        return [other_core(w) for w in ws]

    d1 = ring(d1, "rx")
    d2 = ring(d2, "cb")
    (one, three), (two,) = swapped([d1[0], d1[2]]), swapped([d1[1]])
    d1_other = [one, two, three]
    d2_other = swapped(d2)
    low, high = side[:8, : cols // 16], side[8:, : cols // 16]
    low = [shifted(low, "cb", step) for step in (1, 3)]
    high = [shifted(high, "cb", step) for step in (1, 3)]
    far = [shifted(low[0], "cb", 1)]
    far += [shifted(high[1], "cb", 3)]
    low_other = swapped([side, *low])
    high_other = swapped(high)
    near = [side, low_other[0]]
    for i in range(2):
        near += [low[i], low_other[1 + i], high[i], high_other[i]]
    far_other = swapped(far)
    far = [far[0], far_other[0], far[1], far_other[1]]

    own, *sends = kernel(
        up_part,
        [SMEM] * 3 + [VMEM] + [HBM] * 11,
        jax.ShapeDtypeStruct((few, 2 * part), f32),
        *[jax.ShapeDtypeStruct((few, 2 * part), bf16)] * 3,
        scratch=[
            pltpu.VMEM((n_tok, 2 * part), f32),
            pltpu.VMEM((4, width, 2 * part), bf16),
            pltpu.VMEM((3, n_tok, width), bf16),
            dma((4, 3)),
        ],
    )(core_ref, x_ref, z_ref, x1[0], first_gate, first_up, *x1[1:], *w1, *w1_other)
    got = [shifted(send, "rx", step) for step, send in enumerate(sends, 1)]
    partial = kernel(
        down_part,
        [SMEM] * 2 + [VMEM] * 4 + [HBM] * 8,
        pltpu.VMEM((few, full), bf16),
        scratch=[pltpu.VMEM((part, full), bf16), pltpu.VMEM((16, 16, width), bf16), dma((8,))],
    )(core_ref, x_ref, own, *got, side, first_down, *d1, *d1_other)
    got = exchange(partial.reshape(16, 8, full), ("rz", "cb"))
    send = kernel(
        join,
        [VMEM, HBM],
        jax.ShapeDtypeStruct((16, 8, full + width), bf16),
        scratch=[pltpu.VMEM((16, 16, width), bf16), dma(())],
    )(got, side)
    rows = exchange(send, ("rx", "rz"))
    hidden = kernel(
        ff_near,
        [SMEM, VMEM] + [HBM] * 10,
        jax.ShapeDtypeStruct((3 * part // 4, few), f32),
        scratch=[pltpu.VMEM((few, full), bf16), pltpu.VMEM((16, 6 * part // 4, width), bf16), dma((4, 6))],
    )(core_ref, rows, *near)
    partial = kernel(
        ff_far,
        [SMEM, VMEM, VMEM] + [HBM] * 11,
        pltpu.VMEM((16, few, width), bf16),
        scratch=[
            pltpu.VMEM((few, full), bf16),
            pltpu.VMEM((16, part // 2, width), bf16),
            pltpu.VMEM((part, full), bf16),
            dma((2, 2)),
            dma((7,)),
        ],
    )(core_ref, rows, hidden, second_down, *far, *d2, *d2_other)
    partial, branch = lax.optimization_barrier((partial, second_branch[None]))
    got = exchange(partial, ("rx", "rz"))
    out = kernel(
        finish,
        [VMEM, VMEM, HBM],
        pltpu.VMEM((4, few, width), bf16),
        scratch=[pltpu.VMEM((16, 8, width), bf16), dma((1,))],
    )(got, branch, rows)
    out = exchange(out, "cb")
    return out.reshape(n_tok, width)


def solution(mesh):
    fine = Mesh(mesh.devices.reshape(4, 4, 4, 2), ("rz", "rx", "cb", "dp"))
    ra = ("rz", "rx")
    vector, up, dn = P(ra), P(ra, "cb"), P(("cb", *ra), None)
    layer = (vector, up, up, dn, vector)
    return jax.shard_map(
        shards,
        mesh=fine,
        in_specs=(P("dp", ra), *layer, *layer),
        out_specs=P("dp", ra),
        check_vma=False,
    )
```

```python
import jax
import jax.numpy as jnp
from jax import lax
from jax.experimental import pallas as pl
from jax.experimental.pallas import tpu as pltpu
from jax.sharding import Mesh, PartitionSpec as P

epsilon = 1e-06
residual_scale = 0.25
f32 = jnp.float32
bf16 = jnp.bfloat16
VMEM = pl.BlockSpec(memory_space=pltpu.VMEM)
SMEM = pl.BlockSpec(memory_space=pltpu.SMEM)
HBM = pl.BlockSpec(memory_space=pltpu.HBM)


def exchange(x, axes):
    return lax.all_to_all(x, axes, 0, 0, tiled=True)


def other_core(x):
    return lax.ppermute(x, "dp", [(0, 1), (1, 0)])


def shifted(x, axis, step):
    return lax.ppermute(x, axis, [(i, (i + step) % 4) for i in range(4)])


def dot(a, b, dims):
    return lax.dot_general(a, b, (dims, ((), ())), preferred_element_type=f32)


def silu(v):
    return v / (1.0 + jnp.exp(-v))


def at_lane(core, half):
    return pl.ds(pl.multiple_of(core * half, 128), half)


def together(pairs, sems):
    copies = [pltpu.make_async_copy(*pair, sems.at[i]) for i, pair in enumerate(pairs)]
    for copy in copies:
        copy.start()
    return copies


def wait_for(copies):
    for copy in copies:
        copy.wait()


def pack(core_ref, z_ref, gain, tokens, gate, upward, down1, down2, *refs):
    sends, mine1, mine2, scaled, here, sems = refs[:3], refs[3], refs[4], refs[5], refs[6], refs[7]
    core, z = core_ref[0], z_ref[0]
    rows, wide = sends[0].shape
    part, half = wide // 2, mine1.shape[1]
    pairs = [(tokens, here)]
    for step, send in enumerate(sends, 1):
        at = pl.ds(pl.multiple_of(((z + step) % 4) * part, 128), part)
        for side, w in enumerate((gate, upward)):
            source = w.at[pl.ds(core * rows, rows), at]
            pairs.append((source, send.at[:, pl.ds(side * part, part)]))
    for w, mine in ((down1, mine1), (down2, mine2)):
        pairs.append((w.at[:, at_lane(core, half)], mine))
    copies = together(pairs, sems)
    copies[0].wait()
    scaled[...] = (here[...].astype(f32) * gain[...].astype(f32)).astype(bf16)
    wait_for(copies[1:])


def token_rows(x):
    return [128 * j + 32 * x + 8 * z for z in range(4) for j in range(4)]


def message(core_ref, y_ref, branch, gain, here, tokens, gate, upward, out, picked, sems):
    core, y = core_ref[0], y_ref[0]
    width, cols = picked.shape
    each = cols // 16

    @pl.when(core == 0)
    def _():
        pltpu.make_async_copy(gate, picked, sems.at[16]).start()

    @pl.when(core == 1)
    def _():
        pltpu.make_async_copy(upward, picked, sems.at[16]).start()

    pairs = []
    for z in range(4):
        for x in range(4):
            source = tokens.at[pl.ds(128 * y + 32 * x + 8 * z, 8), :]
            pairs.append((source, out.at[4 * z + x, pl.ds(each, 8), :]))
    copies = together(pairs, sems)
    wide = here[...].astype(f32)
    wide = jnp.concatenate([wide[at : at + 8] for x in range(4) for at in token_rows(x)], 0)
    wide = wide * wide
    turned = (wide[:, :128] + wide[:, 128:]).T
    squares = jnp.broadcast_to(jnp.sum(turned, axis=0, keepdims=True), (8, turned.shape[1]))
    high = squares.astype(bf16).astype(f32)
    mid = (squares - high).astype(bf16).astype(f32)
    low = squares - high - mid
    row = lax.broadcasted_iota(jnp.int32, (8, width), 0)
    fixed = jnp.where(row == 0, branch[...].astype(f32), jnp.where(row == 1, gain[...].astype(f32), 0.0))
    blocks = []
    for x in range(4):
        at = slice(128 * x, 128 * x + 128)
        first = jnp.concatenate([high[:, at], mid[:, at]], 1)
        second = jnp.concatenate([low[:, at], jnp.zeros_like(low[:, at])], 1)
        blocks.append(jnp.where(row == 2, first, jnp.where(row == 3, second, fixed)).astype(bf16))
    pltpu.make_async_copy(gate, picked, sems.at[16]).wait()
    turned = picked[...].T
    for z in range(4):
        for x in range(4):
            to = 4 * z + x
            out[to, :each, :] = turned[to * each : (to + 1) * each, :]
            out[to, each + 8 :, :] = blocks[x]
    wait_for(copies)


def up_part(core_ref, x_ref, z_ref, first_x, gate, upward, *refs):
    xs, mine, other = refs[:3], refs[3:6], refs[6:9]
    own, sends, acc, whole, held, sems = refs[9], refs[10:13], refs[13], refs[14], refs[15], refs[16]
    core, x, z = core_ref[0], x_ref[0], z_ref[0]
    rows, wide = mine[0].shape
    part = wide // 2
    at = pl.ds(pl.multiple_of(z * part, 128), part)
    copies = [[]]
    for side, w in enumerate((gate, upward)):
        copies[0].append((w.at[:, at], whole.at[0, :, pl.ds(side * part, part)]))
    for step in range(3):
        here = (mine[step], whole.at[step + 1, pl.ds(core * rows, rows), :])
        there = (other[step], whole.at[step + 1, pl.ds((1 - core) * rows, rows), :])
        copies.append([here, there, (xs[step], held.at[step])])
    copies = [together(group, sems.at[step]) for step, group in enumerate(copies)]
    total = None
    for step in range(4):
        wait_for(copies[step])
        tokens = held[step - 1] if step else first_x[...]
        one = dot(tokens, whole[step], ((1,), (0,)))
        total = one if total is None else total + one
    acc[...] = total

    def block(to):
        return jnp.concatenate([acc[pl.ds(at, 8), :] for at in token_rows(to)], 0)

    own[...] = block(x)
    for step, send in enumerate(sends, 1):
        send[...] = block((x + step) % 4).astype(bf16)


def down_part(core_ref, x_ref, own, a, b, c, side, w, *refs):
    mine, other, out, whole, small, sems = refs[:3], refs[3:6], refs[6], refs[7], refs[8], refs[9]
    core, x = core_ref[0], x_ref[0]
    rows, full = w.shape
    half = full // 2
    copies = [(side.at[:, pl.ds(rows, 16), :], small), (w, whole.at[pl.ds(x * rows, rows), :])]
    for step in range(1, 4):
        at = pl.ds(((x + 4 - step) % 4) * rows, rows)
        copies.append((mine[step - 1], whole.at[at, at_lane(core, half)]))
        copies.append((other[step - 1], whole.at[at, at_lane(1 - core, half)]))
    copies = together(copies, sems)
    both = own[...] + a[...].astype(f32) + b[...].astype(f32) + c[...].astype(f32)
    copies[0].wait()
    squares = jnp.sum(small[...].astype(f32), axis=0)[10:12]
    squares = squares[0:1, :128] + squares[0:1, 128:] + squares[1:2, :128]
    scale = lax.rsqrt(squares / full + epsilon)
    both = both * jnp.broadcast_to(scale, (8, 128)).T[:, :1]
    part = both.shape[1] // 2
    hidden = (silu(both[:, :part]) * both[:, part:]).astype(bf16)
    wait_for(copies[1:])
    out[...] = dot(hidden, whole[...], ((1,), (0,))).astype(bf16)


def join(got, side, send, small, sem):
    copy = pltpu.make_async_copy(side.at[:, pl.ds(side.shape[1] - 16, 16), :], small, sem)
    copy.start()
    total = jnp.sum(got[...].astype(f32), axis=0)
    copy.wait()
    blocks = [small[i].astype(f32) for i in range(16)]
    tokens, branch, gain = (jnp.concatenate([b[at] for b in blocks], 1) for at in (slice(0, 8), slice(8, 9), slice(9, 10)))
    middle = (residual_scale * tokens + 0.5 * branch * total).astype(bf16)
    mid = middle.astype(f32)
    square = jnp.mean(mid * mid, axis=1, keepdims=True)
    normed = (mid * lax.rsqrt(square + epsilon) * gain).astype(bf16)
    full = normed.shape[1]
    width = full // 16
    for x in range(4):
        for z in range(4):
            block = (4 * z + x) * width
            send[4 * x + z, :, :full] = normed
            send[4 * x + z, :, full:] = middle[:, block : block + width]


def finish(got, branch, send, out, middle, sems):
    count, rows = send.shape[:2]
    width = out.shape[2]
    pairs = [(send.at[:, :, pl.ds(send.shape[2] - width, width)], middle)]
    copies = together(pairs, sems)
    total = jnp.sum(got[...].astype(f32), axis=0)
    wait_for(copies)
    for j in range(count):
        at = slice(j * rows, (j + 1) * rows)
        mid = middle[j].astype(f32)
        value = (residual_scale * mid + 0.5 * branch[...].astype(f32) * total[at]).astype(bf16)
        for y in range(4):
            out[y, at, :] = value


def gated(core, tokens, sources, up, sems):
    blocks, rows, width = up.shape
    cols = rows // (2 * (len(sources) // 2))
    groups = sems.shape[0]
    each = blocks // groups
    pending = []
    for group in range(groups):
        pairs = []
        at = pl.ds(group * each, each)
        for w, slot, side in sources:
            place = 1 - core if side else core
            to = up.at[at, pl.ds(slot * 2 * cols + place * cols, cols), :]
            pairs.append((w.at[at, pl.ds(0, cols), :], to))
        pending.append(together(pairs, sems.at[group]))

    def finish():
        total = None
        for group in range(groups):
            wait_for(pending[group])
            for block in range(group * each, (group + 1) * each):
                part = dot(up[block], tokens[:, block * width : (block + 1) * width], ((1,), (1,)))
                total = part if total is None else total + part
        hidden = []
        for i in range(rows // (2 * cols)):
            gate = total[2 * i * cols : (2 * i + 1) * cols]
            hidden.append(silu(gate) * total[(2 * i + 1) * cols : (2 * i + 2) * cols])
        return jnp.concatenate(hidden, 0)

    return finish


def ff_near(core_ref, got, *refs):
    ups, out, tokens, up, sems = refs[:6], refs[6], refs[7], refs[8], refs[9]
    sources = [(w, i // 2, i % 2) for i, w in enumerate(ups)]
    finish = gated(core_ref[0], tokens, sources, up, sems)
    for j in range(got.shape[0]):
        tokens[8 * j : 8 * j + 8, :] = got[j, :, : tokens.shape[1]]
    out[...] = finish()


def ff_far(core_ref, got, near, w_down, *refs):
    ups, mine, other, out = refs[:2], refs[2:5], refs[5:8], refs[8]
    tokens, up, whole, up_sems, down_sems = refs[9:]
    core = core_ref[0]
    rows, full = w_down.shape
    half = full // 2
    sources = [(ups[0], 0, 0), (ups[1], 0, 1)]
    finish = gated(core, tokens, sources, up, up_sems)
    pairs = [(w_down, whole.at[pl.ds(0, rows), :])]
    for i, piece in enumerate((0, 2, 1), 1):
        at = pl.ds(i * rows, rows)
        pairs.append((mine[piece], whole.at[at, at_lane(core, half)]))
        pairs.append((other[piece], whole.at[at, at_lane(1 - core, half)]))
    copies = together(pairs, down_sems)
    for j in range(got.shape[0]):
        tokens[8 * j : 8 * j + 8, :] = got[j, :, :full]
    hidden = jnp.concatenate([near[...], finish()], 0).T.astype(bf16)
    wait_for(copies)
    width = out.shape[2]
    for z in range(4):
        for x in range(4):
            lanes = slice((4 * z + x) * width, (4 * z + x + 1) * width)
            out[4 * x + z] = dot(hidden, whole[:, lanes], ((1,), (0,))).astype(bf16)


def shards(
    tokens,
    first_gain,
    first_gate,
    first_up,
    first_down,
    first_branch,
    second_gain,
    second_gate,
    second_up,
    second_down,
    second_branch,
):
    core, x, y, z = (lax.axis_index(name) for name in ("dp", "rx", "cb", "rz"))
    core_ref, x_ref, y_ref, z_ref = (i.astype(jnp.int32).reshape(1) for i in (core, x, y, z))
    n_tok, width = tokens.shape
    full = width * 16
    half = width // 2
    cols = first_gate.shape[1]
    part = cols // 4
    few = n_tok // 4
    w_half = jax.ShapeDtypeStruct((first_down.shape[0], full // 2), bf16)

    def kernel(body, ins, *outs, scratch=(), mib=16):
        call = pl.pallas_call(
            body,
            out_shape=list(outs) if len(outs) > 1 else outs[0],
            in_specs=ins,
            out_specs=[VMEM] * len(outs) if len(outs) > 1 else VMEM,
            scratch_shapes=list(scratch),
            compiler_params=pltpu.CompilerParams(vmem_limit_bytes=mib * 2**20),
        )

        def run(*args):
            kept = [pltpu.with_memory_space_constraint(a, pltpu.HBM) if spec is HBM else a for a, spec in zip(args, ins)]
            return call(*kept)

        return run

    dma = pltpu.SemaphoreType.DMA

    *w1, d1, d2, scaled = kernel(
        pack,
        [SMEM] * 2 + [VMEM] + [HBM] * 5,
        *[jax.ShapeDtypeStruct((half, 2 * part), bf16)] * 3,
        w_half,
        w_half,
        jax.ShapeDtypeStruct(tokens.shape, bf16),
        scratch=[pltpu.VMEM(tokens.shape, bf16), dma((9,))],
    )(core_ref, z_ref, first_gain[None], tokens, first_gate, first_up, first_down, second_down)
    w1 = [shifted(w, "rz", step) for step, w in enumerate(w1, 1)]
    x1 = [scaled] + [shifted(scaled, "rz", step) for step in (1, 2, 3)]
    w1_other = [other_core(w) for w in w1]

    side = kernel(
        message,
        [SMEM] * 2 + [VMEM] * 3 + [HBM] * 3,
        jax.ShapeDtypeStruct((16, cols // 16 + 16, width), bf16),
        scratch=[pltpu.VMEM((width, cols), bf16), dma((17,))],
    )(core_ref, y_ref, first_branch[None], second_gain[None], tokens, tokens, second_gate, second_up)
    side = exchange(side, ("rz", "rx"))

    def swapped(ws):
        return [other_core(w) for w in ws]

    d1 = [shifted(d1, "rx", step) for step in (1, 2, 3)]
    d1_other = swapped(d1)
    back, ahead = shifted(d2, "cb", 1), shifted(d2, "cb", 3)
    d2 = [back, shifted(back, "cb", 1), ahead]
    one, three = swapped([back, ahead])
    d2_other = [one, *swapped([d2[1]]), three]
    v1 = side[:, : cols // 16]
    back, ahead = shifted(v1, "cb", 1), shifted(v1, "cb", 3)
    far = [shifted(v1, "cb", 2)]
    near = [side, *swapped([side])]
    one, three = swapped([back, ahead])
    near += [back, one, ahead, three]
    far += swapped(far)

    own, *sends = kernel(
        up_part,
        [SMEM] * 3 + [VMEM] + [HBM] * 11,
        jax.ShapeDtypeStruct((few, 2 * part), f32),
        *[jax.ShapeDtypeStruct((few, 2 * part), bf16)] * 3,
        scratch=[
            pltpu.VMEM((n_tok, 2 * part), f32),
            pltpu.VMEM((4, width, 2 * part), bf16),
            pltpu.VMEM((3, n_tok, width), bf16),
            dma((4, 3)),
        ],
    )(core_ref, x_ref, z_ref, x1[0], first_gate, first_up, *x1[1:], *w1, *w1_other)
    got = [shifted(send, "rx", step) for step, send in enumerate(sends, 1)]
    partial = kernel(
        down_part,
        [SMEM] * 2 + [VMEM] * 4 + [HBM] * 8,
        pltpu.VMEM((few, full), bf16),
        scratch=[pltpu.VMEM((part, full), bf16), pltpu.VMEM((16, 16, width), bf16), dma((8,))],
    )(core_ref, x_ref, own, *got, side, first_down, *d1, *d1_other)
    got = exchange(partial.reshape(16, 8, full), ("rz", "cb"))
    send = kernel(
        join,
        [VMEM, HBM],
        pltpu.VMEM((16, 8, full + width), bf16),
        scratch=[pltpu.VMEM((16, 16, width), bf16), dma(())],
    )(got, side)
    rows = exchange(send, ("rx", "rz"))
    hidden = kernel(
        ff_near,
        [SMEM, VMEM] + [HBM] * 6,
        jax.ShapeDtypeStruct((3 * part // 4, few), f32),
        scratch=[pltpu.VMEM((few, full), bf16), pltpu.VMEM((16, 6 * part // 4, width), bf16), dma((4, 6))],
    )(core_ref, rows, *near)
    partial = kernel(
        ff_far,
        [SMEM, VMEM, VMEM] + [HBM] * 9,
        pltpu.VMEM((16, few, width), bf16),
        scratch=[
            pltpu.VMEM((few, full), bf16),
            pltpu.VMEM((16, part // 2, width), bf16),
            pltpu.VMEM((part, full), bf16),
            dma((2, 2)),
            dma((7,)),
        ],
    )(core_ref, rows, hidden, second_down, *far, *d2, *d2_other)
    partial, branch = lax.optimization_barrier((partial, second_branch[None]))
    got = exchange(partial, ("rx", "rz"))
    out = kernel(
        finish,
        [VMEM, VMEM, HBM],
        pltpu.VMEM((4, few, width), bf16),
        scratch=[pltpu.VMEM((16, 8, width), bf16), dma((1,))],
    )(got, branch, rows)
    out = exchange(out, "cb")
    return out.reshape(n_tok, width)


def solution(mesh):
    fine = Mesh(mesh.devices.reshape(4, 4, 4, 2), ("rz", "rx", "cb", "dp"))
    ra = ("rz", "rx")
    vector, up, dn = P(ra), P(ra, "cb"), P(("cb", *ra), None)
    layer = (vector, up, up, dn, vector)
    return jax.shard_map(
        shards,
        mesh=fine,
        in_specs=(P("dp", ra), *layer, *layer),
        out_specs=P("dp", ra),
        check_vma=False,
    )
```

```python
import jax
import jax.numpy as jnp
from jax import lax
from jax.experimental import pallas as pl
from jax.experimental.pallas import tpu as pltpu
from jax.sharding import Mesh, PartitionSpec as P

epsilon = 1e-06
residual_scale = 0.25
f32 = jnp.float32
bf16 = jnp.bfloat16
VMEM = pl.BlockSpec(memory_space=pltpu.VMEM)
SMEM = pl.BlockSpec(memory_space=pltpu.SMEM)
HBM = pl.BlockSpec(memory_space=pltpu.HBM)


def exchange(x, axes):
    return lax.all_to_all(x, axes, 0, 0, tiled=True)


def other_core(x):
    return lax.ppermute(x, "dp", [(0, 1), (1, 0)])


def shifted(x, axis, step):
    return lax.ppermute(x, axis, [(i, (i + step) % 4) for i in range(4)])


def dot(a, b, dims):
    return lax.dot_general(a, b, (dims, ((), ())), preferred_element_type=f32)


def silu(v):
    return v / (1.0 + jnp.exp(-v))


def at_lane(core, half):
    return pl.ds(pl.multiple_of(core * half, 128), half)


def together(pairs, sems):
    copies = [pltpu.make_async_copy(*pair, sems.at[i]) for i, pair in enumerate(pairs)]
    for copy in copies:
        copy.start()
    return copies


def wait_for(copies):
    for copy in copies:
        copy.wait()


def pack(core_ref, z_ref, gain, tokens, gate, upward, down1, down2, *refs):
    sends, mine1, mine2, scaled, here, sems = refs[:3], refs[3], refs[4], refs[5], refs[6], refs[7]
    core, z = core_ref[0], z_ref[0]
    rows, wide = sends[0].shape
    part, half = wide // 2, mine1.shape[1]
    pairs = [(tokens, here)]
    for step, send in enumerate(sends, 1):
        at = pl.ds(pl.multiple_of(((z + step) % 4) * part, 128), part)
        for side, w in enumerate((gate, upward)):
            source = w.at[pl.ds(core * rows, rows), at]
            pairs.append((source, send.at[:, pl.ds(side * part, part)]))
    for w, mine in ((down1, mine1), (down2, mine2)):
        pairs.append((w.at[:, at_lane(core, half)], mine))
    copies = together(pairs, sems)
    copies[0].wait()
    scaled[...] = (here[...].astype(f32) * gain[...].astype(f32).reshape(1, -1)).astype(bf16)
    wait_for(copies[1:])


def message(core_ref, y_ref, branch, gain, here, tokens, gate, upward, out, picked, sems):
    core, y = core_ref[0], y_ref[0]
    width, cols = picked.shape
    each = cols // 16

    @pl.when(core == 0)
    def _():
        pltpu.make_async_copy(gate, picked, sems.at[16]).start()

    @pl.when(core == 1)
    def _():
        pltpu.make_async_copy(upward, picked, sems.at[16]).start()

    pairs = []
    for z in range(4):
        for x in range(4):
            source = tokens.at[pl.ds(x * 128 + 32 * z + 8 * y, 8), :]
            pairs.append((source, out.at[4 * z + x, pl.ds(each, 8), :]))
    copies = together(pairs, sems)
    wide = here[...].astype(f32)
    squares = lax.dot_general(
        jnp.ones((8, width), f32),
        wide * wide,
        (((1,), (1,)), ((), ())),
        precision=lax.Precision.HIGHEST,
        preferred_element_type=f32,
    )
    high = squares.astype(bf16).astype(f32)
    mid = (squares - high).astype(bf16).astype(f32)
    low = squares - high - mid
    row = lax.broadcasted_iota(jnp.int32, (8, width), 0)
    fixed = jnp.where(row == 0, branch[...].astype(f32), jnp.where(row == 1, gain[...].astype(f32), 0.0))
    blocks = []
    for x in range(4):
        at = slice(128 * x, 128 * x + 128)
        first = jnp.concatenate([high[:, at], mid[:, at]], 1)
        second = jnp.concatenate([low[:, at], jnp.zeros_like(low[:, at])], 1)
        blocks.append(jnp.where(row == 2, first, jnp.where(row == 3, second, fixed)).astype(bf16))
    pltpu.make_async_copy(gate, picked, sems.at[16]).wait()
    turned = picked[...].T
    for z in range(4):
        for x in range(4):
            to = 4 * z + x
            out[to, :each, :] = turned[to * each : (to + 1) * each, :]
            out[to, each + 8 :, :] = blocks[x]
    wait_for(copies)


def up_part(core_ref, x_ref, z_ref, first_x, gate, upward, *refs):
    xs, mine, other = refs[:3], refs[3:6], refs[6:9]
    own, sends, acc, whole, held, sems = refs[9], refs[10:13], refs[13], refs[14], refs[15], refs[16]
    core, x, z = core_ref[0], x_ref[0], z_ref[0]
    rows, wide = mine[0].shape
    part = wide // 2
    at = pl.ds(pl.multiple_of(z * part, 128), part)
    copies = [[]]
    for side, w in enumerate((gate, upward)):
        copies[0].append((w.at[:, at], whole.at[0, :, pl.ds(side * part, part)]))
    for step in range(3):
        here = (mine[step], whole.at[step + 1, pl.ds(core * rows, rows), :])
        there = (other[step], whole.at[step + 1, pl.ds((1 - core) * rows, rows), :])
        copies.append([here, there, (xs[step], held.at[step])])
    copies = [together(group, sems.at[step]) for step, group in enumerate(copies)]
    total = None
    for step in range(4):
        wait_for(copies[step])
        tokens = held[step - 1] if step else first_x[...]
        one = dot(tokens, whole[step], ((1,), (0,)))
        total = one if total is None else total + one
    acc[...] = total
    own[...] = acc[pl.ds(x * 128, 128), :]
    for step, send in enumerate(sends, 1):
        send[...] = acc[pl.ds(((x + step) % 4) * 128, 128), :].astype(bf16)


def down_part(core_ref, x_ref, own, a, b, c, side, w, *refs):
    mine, other, out, whole, small, sems = refs[:3], refs[3:6], refs[6], refs[7], refs[8], refs[9]
    core, x = core_ref[0], x_ref[0]
    rows, full = w.shape
    half = full // 2
    copies = [(side.at[:, pl.ds(rows, 16), :], small), (w, whole.at[pl.ds(x * rows, rows), :])]
    for step in range(1, 4):
        at = pl.ds(((x + 4 - step) % 4) * rows, rows)
        copies.append((mine[step - 1], whole.at[at, at_lane(core, half)]))
        copies.append((other[step - 1], whole.at[at, at_lane(1 - core, half)]))
    copies = together(copies, sems)
    both = own[...] + a[...].astype(f32) + b[...].astype(f32) + c[...].astype(f32)
    copies[0].wait()
    squares = jnp.sum(small[...].astype(f32), axis=0)[10:12]
    squares = squares[0:1, :128] + squares[0:1, 128:] + squares[1:2, :128]
    scale = lax.rsqrt(squares / full + epsilon)
    both = both * jnp.broadcast_to(scale, (8, 128)).T[:, :1]
    part = both.shape[1] // 2
    hidden = (silu(both[:, :part]) * both[:, part:]).astype(bf16)
    wait_for(copies[1:])
    out[...] = dot(hidden, whole[...], ((1,), (0,))).astype(bf16)


def join(got, side, send, small, sem):
    copy = pltpu.make_async_copy(side.at[:, pl.ds(side.shape[1] - 16, 16), :], small, sem)
    copy.start()
    total = jnp.sum(got[...].astype(f32), axis=0)
    copy.wait()
    blocks = [small[i].astype(f32) for i in range(16)]
    tokens, branch, gain = (jnp.concatenate([b[at] for b in blocks], 1) for at in (slice(0, 8), slice(8, 9), slice(9, 10)))
    middle = (residual_scale * tokens + 0.5 * branch * total).astype(bf16)
    mid = middle.astype(f32)
    square = jnp.mean(mid * mid, axis=1, keepdims=True)
    normed = (mid * lax.rsqrt(square + epsilon) * gain).astype(bf16)
    full = normed.shape[1]
    width = full // 16
    for x in range(4):
        for z in range(4):
            block = (4 * z + x) * width
            send[4 * x + z, :, :full] = normed
            send[4 * x + z, :, full:] = middle[:, block : block + width]


def finish(got, branch, send, out, middle, sems):
    count, rows = send.shape[:2]
    width = out.shape[2]
    pairs = [(send.at[:, :, pl.ds(send.shape[2] - width, width)], middle)]
    copies = together(pairs, sems)
    total = jnp.sum(got[...].astype(f32), axis=0)
    wait_for(copies)
    for j in range(count):
        at = slice(j * rows, (j + 1) * rows)
        mid = middle[j].astype(f32)
        value = (residual_scale * mid + 0.5 * branch[...].astype(f32) * total[at]).astype(bf16)
        for y in range(4):
            out[y, at, :] = value


def feed_forward(core_ref, got, w_down, *refs):
    ups, mine, other, out = refs[:8], refs[8:11], refs[11:14], refs[14]
    tokens, up, whole, up_sems, down_sems = refs[15:]
    core = core_ref[0]
    blocks, cols, width = ups[0].shape
    rows, full = w_down.shape
    half = full // 2
    groups = up_sems.shape[0]
    each = blocks // groups
    up_copies = []
    for group in range(groups):
        at = pl.ds(group * each, each)
        copies = []
        for step in range(4):
            for side, place in enumerate((core, 1 - core)):
                to = up.at[at, pl.ds(step * 2 * cols + place * cols, cols), :]
                source = ups[2 * step + side].at[at]
                copies.append(pltpu.make_async_copy(source, to, up_sems.at[group, 2 * step + side]))
        up_copies.append(copies)
    down_copies = [(w_down, whole.at[pl.ds(0, rows), :])]
    for step in range(1, 4):
        at = pl.ds(step * rows, rows)
        down_copies.append((mine[step - 1], whole.at[at, at_lane(core, half)]))
        down_copies.append((other[step - 1], whole.at[at, at_lane(1 - core, half)]))
    down_copies = [pltpu.make_async_copy(*c, down_sems.at[i]) for i, c in enumerate(down_copies)]
    for copy in [c for copies in up_copies for c in copies] + down_copies:
        copy.start()
    for j in range(got.shape[0]):
        tokens[8 * j : 8 * j + 8, :] = got[j, :, :full]
    total = None
    for group in range(groups):
        for copy in up_copies[group]:
            copy.wait()
        for block in range(group * each, (group + 1) * each):
            part = dot(up[block], tokens[:, block * width : (block + 1) * width], ((1,), (1,)))
            total = part if total is None else total + part
    hidden = []
    for step in range(4):
        gate = total[2 * step * cols : (2 * step + 1) * cols]
        upward = total[(2 * step + 1) * cols : (2 * step + 2) * cols]
        hidden.append(silu(gate) * upward)
    hidden = jnp.concatenate(hidden, 0).T.astype(bf16)
    for copy in down_copies:
        copy.wait()
    for block in range(blocks):
        lanes = slice(block * width, (block + 1) * width)
        out[block] = dot(hidden, whole[:, lanes], ((1,), (0,))).astype(bf16)


def shards(
    tokens,
    first_gain,
    first_gate,
    first_up,
    first_down,
    first_branch,
    second_gain,
    second_gate,
    second_up,
    second_down,
    second_branch,
):
    core, x, y, z = (lax.axis_index(name) for name in ("dp", "rx", "cb", "rz"))
    core_ref, x_ref, y_ref, z_ref = (i.astype(jnp.int32).reshape(1) for i in (core, x, y, z))
    n_tok, width = tokens.shape
    full = width * 16
    half = width // 2
    cols = first_gate.shape[1]
    part = cols // 4
    few = n_tok // 4
    w_half = jax.ShapeDtypeStruct((first_down.shape[0], full // 2), bf16)

    def kernel(body, ins, *outs, scratch=(), mib=16):
        call = pl.pallas_call(
            body,
            out_shape=list(outs) if len(outs) > 1 else outs[0],
            in_specs=ins,
            out_specs=[VMEM] * len(outs) if len(outs) > 1 else VMEM,
            scratch_shapes=list(scratch),
            compiler_params=pltpu.CompilerParams(vmem_limit_bytes=mib * 2**20),
        )

        def run(*args):
            kept = [pltpu.with_memory_space_constraint(a, pltpu.HBM) if spec is HBM else a for a, spec in zip(args, ins)]
            return call(*kept)

        return run

    dma = pltpu.SemaphoreType.DMA

    *w1, d1, d2, scaled = kernel(
        pack,
        [SMEM] * 2 + [VMEM] + [HBM] * 5,
        *[jax.ShapeDtypeStruct((half, 2 * part), bf16)] * 3,
        w_half,
        w_half,
        jax.ShapeDtypeStruct(tokens.shape, bf16),
        scratch=[pltpu.VMEM(tokens.shape, bf16), dma((9,))],
    )(core_ref, z_ref, first_gain, tokens, first_gate, first_up, first_down, second_down)
    w1 = [shifted(w, "rz", step) for step, w in enumerate(w1, 1)]
    x1 = [scaled] + [shifted(scaled, "rz", step) for step in (1, 2, 3)]
    w1_other = [other_core(w) for w in w1]

    side = kernel(
        message,
        [SMEM] * 2 + [VMEM] * 3 + [HBM] * 3,
        jax.ShapeDtypeStruct((16, cols // 16 + 16, width), bf16),
        scratch=[pltpu.VMEM((width, cols), bf16), dma((17,))],
    )(core_ref, y_ref, first_branch[None], second_gain[None], tokens, tokens, second_gate, second_up)
    side = exchange(side, ("rz", "rx"))
    v1 = side[:, : cols // 16]

    d1 = [shifted(d1, "rx", step) for step in (1, 2, 3)]
    d2 = [shifted(d2, "cb", step) for step in (1, 2, 3)]
    near = [shifted(v1, "cb", step) for step in (1, 3)]
    v1 = [v1, near[0], shifted(v1, "cb", 2), near[1]]
    d1_other = [other_core(w) for w in d1]
    d2_other = [other_core(w) for w in d2]
    v1 = [w for mine in v1 for w in (mine, other_core(mine))]

    own, *sends = kernel(
        up_part,
        [SMEM] * 3 + [VMEM] + [HBM] * 11,
        jax.ShapeDtypeStruct((few, 2 * part), f32),
        *[jax.ShapeDtypeStruct((few, 2 * part), bf16)] * 3,
        scratch=[
            pltpu.VMEM((n_tok, 2 * part), f32),
            pltpu.VMEM((4, width, 2 * part), bf16),
            pltpu.VMEM((3, n_tok, width), bf16),
            dma((4, 3)),
        ],
    )(core_ref, x_ref, z_ref, x1[0], first_gate, first_up, *x1[1:], *w1, *w1_other)
    got = [shifted(send, "rx", step) for step, send in enumerate(sends, 1)]
    partial = kernel(
        down_part,
        [SMEM] * 2 + [VMEM] * 4 + [HBM] * 8,
        pltpu.VMEM((few, full), bf16),
        scratch=[pltpu.VMEM((part, full), bf16), pltpu.VMEM((16, 16, width), bf16), dma((8,))],
    )(core_ref, x_ref, own, *got, side, first_down, *d1, *d1_other)
    got = exchange(partial.reshape(16, 8, full), ("rz", "cb"))
    send = kernel(
        join,
        [VMEM, HBM],
        jax.ShapeDtypeStruct((16, 8, full + width), bf16),
        scratch=[pltpu.VMEM((16, 16, width), bf16), dma(())],
    )(got, side)
    rows = exchange(send, ("rx", "rz"))
    partial = kernel(
        feed_forward,
        [SMEM, VMEM] + [HBM] * 15,
        pltpu.VMEM((16, few, width), bf16),
        scratch=[
            pltpu.VMEM((few, full), bf16),
            pltpu.VMEM((16, 2 * part, width), bf16),
            pltpu.VMEM((part, full), bf16),
            dma((4, 8)),
            dma((7,)),
        ],
        mib=24,
    )(core_ref, rows, second_down, *v1, *d2, *d2_other)
    partial, branch = lax.optimization_barrier((partial, second_branch[None]))
    got = exchange(partial, ("rz", "rx"))
    out = kernel(
        finish,
        [VMEM, VMEM, HBM],
        pltpu.VMEM((4, few, width), bf16),
        scratch=[pltpu.VMEM((16, 8, width), bf16), dma((1,))],
    )(got, branch, rows)
    out = exchange(out, "cb")
    return out.reshape(4, 16, 8, width).transpose(1, 0, 2, 3).reshape(n_tok, width)


def solution(mesh):
    fine = Mesh(mesh.devices.reshape(4, 4, 4, 2), ("rz", "rx", "cb", "dp"))
    ra = ("rz", "rx")
    vector, up, dn = P(ra), P(ra, "cb"), P(("cb", *ra), None)
    layer = (vector, up, up, dn, vector)
    return jax.shard_map(
        shards,
        mesh=fine,
        in_specs=(P("dp", ra), *layer, *layer),
        out_specs=P("dp", ra),
        check_vma=False,
    )
```

```python
import jax
import jax.numpy as jnp
from jax import lax
from jax.experimental import pallas as pl
from jax.experimental.pallas import tpu as pltpu
from jax.sharding import Mesh, PartitionSpec as P

epsilon = 1e-06
residual_scale = 0.25
f32 = jnp.float32
bf16 = jnp.bfloat16
VMEM = pl.BlockSpec(memory_space=pltpu.VMEM)
SMEM = pl.BlockSpec(memory_space=pltpu.SMEM)
HBM = pl.BlockSpec(memory_space=pltpu.HBM)
ANY = pl.BlockSpec(memory_space=pl.ANY)


def exchange(x, axes):
    return lax.all_to_all(x, axes, 0, 0, tiled=True)


def other_core(x):
    return lax.ppermute(x, "dp", [(0, 1), (1, 0)])


def shifted(x, axis, step):
    return lax.ppermute(x, axis, [(i, (i + step) % 4) for i in range(4)])


def dot(a, b, dims):
    return lax.dot_general(a, b, (dims, ((), ())), preferred_element_type=f32)


def silu(v):
    return v / (1.0 + jnp.exp(-v))


def at_lane(core, half):
    return pl.ds(pl.multiple_of(core * half, 128), half)


def together(pairs, sems):
    copies = [pltpu.make_async_copy(*pair, sems.at[i]) for i, pair in enumerate(pairs)]
    for copy in copies:
        copy.start()
    return copies


def wait_for(copies):
    for copy in copies:
        copy.wait()


def pack(core_ref, z_ref, gain, tokens, gate, upward, down1, down2, *refs):
    sends, mine1, mine2, scaled, here, sems = refs[:3], refs[3], refs[4], refs[5], refs[6], refs[7]
    core, z = core_ref[0], z_ref[0]
    rows, wide = sends[0].shape
    part, half = wide // 2, mine1.shape[1]
    pairs = [(tokens, here)]
    for step, send in enumerate(sends, 1):
        at = pl.ds(pl.multiple_of(((z + step) % 4) * part, 128), part)
        for side, w in enumerate((gate, upward)):
            source = w.at[pl.ds(core * rows, rows), at]
            pairs.append((source, send.at[:, pl.ds(side * part, part)]))
    for w, mine in ((down1, mine1), (down2, mine2)):
        pairs.append((w.at[:, at_lane(core, half)], mine))
    copies = together(pairs, sems)
    copies[0].wait()
    scaled[...] = (here[...].astype(f32) * gain[...].astype(f32).reshape(1, -1)).astype(bf16)
    wait_for(copies[1:])


def message(core_ref, y_ref, branch, gain, here, tokens, gate, upward, out, picked, sems):
    core, y = core_ref[0], y_ref[0]
    width, cols = picked.shape
    each = cols // 16

    @pl.when(core == 0)
    def _():
        pltpu.make_async_copy(gate, picked, sems.at[16]).start()

    @pl.when(core == 1)
    def _():
        pltpu.make_async_copy(upward, picked, sems.at[16]).start()

    pairs = []
    for z in range(4):
        for x in range(4):
            source = tokens.at[pl.ds(x * 128 + 32 * z + 8 * y, 8), :]
            pairs.append((source, out.at[4 * z + x, pl.ds(each, 8), :]))
    copies = together(pairs, sems)
    wide = here[...].astype(f32)
    squares = lax.dot_general(
        jnp.ones((8, width), f32),
        wide * wide,
        (((1,), (1,)), ((), ())),
        precision=lax.Precision.HIGHEST,
        preferred_element_type=f32,
    )
    high = squares.astype(bf16).astype(f32)
    mid = (squares - high).astype(bf16).astype(f32)
    low = squares - high - mid
    row = lax.broadcasted_iota(jnp.int32, (8, width), 0)
    fixed = jnp.where(row == 0, branch[...].astype(f32), jnp.where(row == 1, gain[...].astype(f32), 0.0))
    blocks = []
    for x in range(4):
        at = slice(128 * x, 128 * x + 128)
        first = jnp.concatenate([high[:, at], mid[:, at]], 1)
        second = jnp.concatenate([low[:, at], jnp.zeros_like(low[:, at])], 1)
        blocks.append(jnp.where(row == 2, first, jnp.where(row == 3, second, fixed)).astype(bf16))
    pltpu.make_async_copy(gate, picked, sems.at[16]).wait()
    turned = picked[...].T
    for z in range(4):
        for x in range(4):
            to = 4 * z + x
            out[to, :each, :] = turned[to * each : (to + 1) * each, :]
            out[to, each + 8 :, :] = blocks[x]
    wait_for(copies)


def up_part(core_ref, x_ref, z_ref, first_x, gate, upward, *refs):
    xs, mine, other = refs[:3], refs[3:6], refs[6:9]
    own, sends, acc, whole, held, sems = refs[9], refs[10:13], refs[13], refs[14], refs[15], refs[16]
    core, x, z = core_ref[0], x_ref[0], z_ref[0]
    rows, wide = mine[0].shape
    part = wide // 2
    at = pl.ds(pl.multiple_of(z * part, 128), part)
    copies = [[]]
    for side, w in enumerate((gate, upward)):
        copies[0].append((w.at[:, at], whole.at[0, :, pl.ds(side * part, part)]))
    for step in range(3):
        here = (mine[step], whole.at[step + 1, pl.ds(core * rows, rows), :])
        there = (other[step], whole.at[step + 1, pl.ds((1 - core) * rows, rows), :])
        copies.append([here, there, (xs[step], held.at[step])])
    copies = [together(group, sems.at[step]) for step, group in enumerate(copies)]
    total = None
    for step in range(4):
        wait_for(copies[step])
        tokens = held[step - 1] if step else first_x[...]
        one = dot(tokens, whole[step], ((1,), (0,)))
        total = one if total is None else total + one
    acc[...] = total
    own[...] = acc[pl.ds(x * 128, 128), :]
    for step, send in enumerate(sends, 1):
        send[...] = acc[pl.ds(((x + step) % 4) * 128, 128), :].astype(bf16)


def down_part(core_ref, x_ref, own, a, b, c, side, w, *refs):
    mine, other, out, whole, small, sems = refs[:3], refs[3:6], refs[6], refs[7], refs[8], refs[9]
    core, x = core_ref[0], x_ref[0]
    rows, full = w.shape
    half = full // 2
    copies = [(side.at[:, pl.ds(rows, 16), :], small), (w, whole.at[pl.ds(x * rows, rows), :])]
    for step in range(1, 4):
        at = pl.ds(((x + 4 - step) % 4) * rows, rows)
        copies.append((mine[step - 1], whole.at[at, at_lane(core, half)]))
        copies.append((other[step - 1], whole.at[at, at_lane(1 - core, half)]))
    copies = together(copies, sems)
    both = own[...] + a[...].astype(f32) + b[...].astype(f32) + c[...].astype(f32)
    copies[0].wait()
    squares = jnp.sum(small[...].astype(f32), axis=0)[10:12]
    squares = squares[0:1, :128] + squares[0:1, 128:] + squares[1:2, :128]
    scale = lax.rsqrt(squares / full + epsilon)
    both = both * jnp.broadcast_to(scale, (8, 128)).T[:, :1]
    part = both.shape[1] // 2
    hidden = (silu(both[:, :part]) * both[:, part:]).astype(bf16)
    wait_for(copies[1:])
    out[...] = dot(hidden, whole[...], ((1,), (0,))).astype(bf16)


def join(got, side, send, small, sem):
    copy = pltpu.make_async_copy(side.at[:, pl.ds(side.shape[1] - 16, 16), :], small, sem)
    copy.start()
    total = jnp.sum(got[...].astype(f32), axis=0)
    copy.wait()
    blocks = [small[i].astype(f32) for i in range(16)]
    tokens, branch, gain = (jnp.concatenate([b[at] for b in blocks], 1) for at in (slice(0, 8), slice(8, 9), slice(9, 10)))
    middle = (residual_scale * tokens + 0.5 * branch * total).astype(bf16)
    mid = middle.astype(f32)
    square = jnp.mean(mid * mid, axis=1, keepdims=True)
    normed = (mid * lax.rsqrt(square + epsilon) * gain).astype(bf16)
    full = normed.shape[1]
    width = full // 16
    for x in range(4):
        for z in range(4):
            block = (4 * z + x) * width
            send[4 * x + z, :, :full] = normed
            send[4 * x + z, :, full:] = middle[:, block : block + width]


def finish(got, branch, send, out, middle, sems):
    count, rows = send.shape[:2]
    width = out.shape[2]
    pairs = [(send.at[:, :, pl.ds(send.shape[2] - width, width)], middle)]
    copies = together(pairs, sems)
    total = jnp.sum(got[...].astype(f32), axis=0)
    wait_for(copies)
    for j in range(count):
        at = slice(j * rows, (j + 1) * rows)
        mid = middle[j].astype(f32)
        value = (residual_scale * mid + 0.5 * branch[...].astype(f32) * total[at]).astype(bf16)
        for y in range(4):
            out[y, at, :] = value


def feed_forward(core_ref, got, w_down, *refs):
    ups, mine, other, out = refs[:8], refs[8:11], refs[11:14], refs[14]
    tokens, up, whole, up_sems, down_sems = refs[15:]
    core = core_ref[0]
    blocks, cols, width = ups[0].shape
    rows, full = w_down.shape
    half = full // 2
    groups = up_sems.shape[0]
    each = blocks // groups
    up_copies = []
    for group in range(groups):
        at = pl.ds(group * each, each)
        copies = []
        for step in range(4):
            for side, place in enumerate((core, 1 - core)):
                to = up.at[at, pl.ds(step * 2 * cols + place * cols, cols), :]
                source = ups[2 * step + side].at[at]
                copies.append(pltpu.make_async_copy(source, to, up_sems.at[group, 2 * step + side]))
        up_copies.append(copies)
    down_copies = [(w_down, whole.at[pl.ds(0, rows), :])]
    for step in range(1, 4):
        at = pl.ds(step * rows, rows)
        down_copies.append((mine[step - 1], whole.at[at, at_lane(core, half)]))
        down_copies.append((other[step - 1], whole.at[at, at_lane(1 - core, half)]))
    down_copies = [pltpu.make_async_copy(*c, down_sems.at[i]) for i, c in enumerate(down_copies)]
    for copy in [c for copies in up_copies for c in copies] + down_copies:
        copy.start()
    for j in range(got.shape[0]):
        tokens[8 * j : 8 * j + 8, :] = got[j, :, :full]
    total = None
    for group in range(groups):
        for copy in up_copies[group]:
            copy.wait()
        for block in range(group * each, (group + 1) * each):
            part = dot(up[block], tokens[:, block * width : (block + 1) * width], ((1,), (1,)))
            total = part if total is None else total + part
    hidden = []
    for step in range(4):
        gate = total[2 * step * cols : (2 * step + 1) * cols]
        upward = total[(2 * step + 1) * cols : (2 * step + 2) * cols]
        hidden.append(silu(gate) * upward)
    hidden = jnp.concatenate(hidden, 0).T.astype(bf16)
    for copy in down_copies:
        copy.wait()
    for block in range(blocks):
        lanes = slice(block * width, (block + 1) * width)
        out[block] = dot(hidden, whole[:, lanes], ((1,), (0,))).astype(bf16)


def shards(
    tokens,
    first_gain,
    first_gate,
    first_up,
    first_down,
    first_branch,
    second_gain,
    second_gate,
    second_up,
    second_down,
    second_branch,
):
    core, x, y, z = (lax.axis_index(name) for name in ("dp", "rx", "cb", "rz"))
    core_ref, x_ref, y_ref, z_ref = (i.astype(jnp.int32).reshape(1) for i in (core, x, y, z))
    n_tok, width = tokens.shape
    full = width * 16
    half = width // 2
    cols = first_gate.shape[1]
    part = cols // 4
    few = n_tok // 4
    w_half = jax.ShapeDtypeStruct((first_down.shape[0], full // 2), bf16)

    def kernel(body, ins, *outs, scratch=(), mib=16):
        call = pl.pallas_call(
            body,
            out_shape=list(outs) if len(outs) > 1 else outs[0],
            in_specs=ins,
            out_specs=[VMEM] * len(outs) if len(outs) > 1 else VMEM,
            scratch_shapes=list(scratch),
            compiler_params=pltpu.CompilerParams(vmem_limit_bytes=mib * 2**20),
        )

        def run(*args):
            kept = [pltpu.with_memory_space_constraint(a, pltpu.HBM) if spec is HBM else a for a, spec in zip(args, ins)]
            return call(*kept)

        return run

    dma = pltpu.SemaphoreType.DMA

    *w1, d1, d2, scaled = kernel(
        pack,
        [SMEM] * 2 + [VMEM] + [HBM] * 5,
        *[jax.ShapeDtypeStruct((half, 2 * part), bf16)] * 3,
        w_half,
        w_half,
        jax.ShapeDtypeStruct(tokens.shape, bf16),
        scratch=[pltpu.VMEM(tokens.shape, bf16), dma((9,))],
    )(core_ref, z_ref, first_gain, tokens, first_gate, first_up, first_down, second_down)
    w1 = [shifted(w, "rz", step) for step, w in enumerate(w1, 1)]
    x1 = [scaled] + [shifted(scaled, "rz", step) for step in (1, 2, 3)]
    w1_other = [other_core(w) for w in w1]

    side = kernel(
        message,
        [SMEM] * 2 + [VMEM] * 3 + [HBM] * 3,
        jax.ShapeDtypeStruct((16, cols // 16 + 16, width), bf16),
        scratch=[pltpu.VMEM((width, cols), bf16), dma((17,))],
    )(core_ref, y_ref, first_branch[None], second_gain[None], tokens, tokens, second_gate, second_up)
    side = exchange(side, ("rz", "rx"))
    v1 = side[:, : cols // 16]

    d1 = [shifted(d1, "rx", step) for step in (1, 2, 3)]
    d2 = [shifted(d2, "cb", step) for step in (1, 2, 3)]
    near = [shifted(v1, "cb", step) for step in (1, 3)]
    v1 = [v1, near[0], shifted(v1, "cb", 2), near[1]]
    d1_other = [other_core(w) for w in d1]
    d2_other = [other_core(w) for w in d2]
    v1 = [w for mine in v1 for w in (mine, other_core(mine))]

    own, *sends = kernel(
        up_part,
        [SMEM] * 3 + [VMEM] + [HBM] * 2 + [ANY] * 9,
        jax.ShapeDtypeStruct((few, 2 * part), f32),
        *[jax.ShapeDtypeStruct((few, 2 * part), bf16)] * 3,
        scratch=[
            pltpu.VMEM((n_tok, 2 * part), f32),
            pltpu.VMEM((4, width, 2 * part), bf16),
            pltpu.VMEM((3, n_tok, width), bf16),
            dma((4, 3)),
        ],
    )(core_ref, x_ref, z_ref, x1[0], first_gate, first_up, *x1[1:], *w1, *w1_other)
    got = [shifted(send, "rx", step) for step, send in enumerate(sends, 1)]
    partial = kernel(
        down_part,
        [SMEM] * 2 + [VMEM] * 4 + [HBM] * 5 + [ANY] * 3,
        pltpu.VMEM((few, full), bf16),
        scratch=[pltpu.VMEM((part, full), bf16), pltpu.VMEM((16, 16, width), bf16), dma((8,))],
    )(core_ref, x_ref, own, *got, side, first_down, *d1, *d1_other)
    got = exchange(partial.reshape(16, 8, full), ("rz", "cb"))
    send = kernel(
        join,
        [VMEM, HBM],
        jax.ShapeDtypeStruct((16, 8, full + width), bf16),
        scratch=[pltpu.VMEM((16, 16, width), bf16), dma(())],
    )(got, side)
    rows = exchange(send, ("rx", "rz"))
    partial = kernel(
        feed_forward,
        [SMEM, VMEM] + [HBM] * 4 + [ANY] * 3 + [HBM, ANY] + [HBM] * 6,
        pltpu.VMEM((16, few, width), bf16),
        scratch=[
            pltpu.VMEM((few, full), bf16),
            pltpu.VMEM((16, 2 * part, width), bf16),
            pltpu.VMEM((part, full), bf16),
            dma((4, 8)),
            dma((7,)),
        ],
        mib=24,
    )(core_ref, rows, second_down, *v1, *d2, *d2_other)
    partial, branch = lax.optimization_barrier((partial, second_branch[None]))
    got = exchange(partial, ("rz", "rx"))
    out = kernel(
        finish,
        [VMEM, VMEM, HBM],
        pltpu.VMEM((4, few, width), bf16),
        scratch=[pltpu.VMEM((16, 8, width), bf16), dma((1,))],
    )(got, branch, rows)
    out = exchange(out, "cb")
    return out.reshape(4, 16, 8, width).transpose(1, 0, 2, 3).reshape(n_tok, width)


def solution(mesh):
    fine = Mesh(mesh.devices.reshape(4, 4, 4, 2), ("rz", "rx", "cb", "dp"))
    ra = ("rz", "rx")
    vector, up, dn = P(ra), P(ra, "cb"), P(("cb", *ra), None)
    layer = (vector, up, up, dn, vector)
    return jax.shard_map(
        shards,
        mesh=fine,
        in_specs=(P("dp", ra), *layer, *layer),
        out_specs=P("dp", ra),
        check_vma=False,
    )
```

```python
import jax
import jax.numpy as jnp
from jax import lax
from jax.experimental import pallas as pl
from jax.experimental.pallas import tpu as pltpu
from jax.sharding import Mesh, PartitionSpec as P

epsilon = 1e-06
residual_scale = 0.25
f32 = jnp.float32
bf16 = jnp.bfloat16
VMEM = pl.BlockSpec(memory_space=pltpu.VMEM)
SMEM = pl.BlockSpec(memory_space=pltpu.SMEM)
HBM = pl.BlockSpec(memory_space=pltpu.HBM)
ANY = pl.BlockSpec(memory_space=pl.ANY)


def exchange(x, axes):
    return lax.all_to_all(x, axes, 0, 0, tiled=True)


def other_core(x):
    return lax.ppermute(x, "dp", [(0, 1), (1, 0)])


def shifted(x, axis, step):
    return lax.ppermute(x, axis, [(i, (i + step) % 4) for i in range(4)])


def dot(a, b, dims):
    return lax.dot_general(a, b, (dims, ((), ())), preferred_element_type=f32)


def silu(v):
    return v / (1.0 + jnp.exp(-v))


def at_lane(core, half):
    return pl.ds(pl.multiple_of(core * half, 128), half)


def together(pairs, sems):
    copies = [pltpu.make_async_copy(*pair, sems.at[i]) for i, pair in enumerate(pairs)]
    for copy in copies:
        copy.start()
    return copies


def wait_for(copies):
    for copy in copies:
        copy.wait()


def pack(core_ref, z_ref, gain, tokens, gate, upward, down1, down2, *refs):
    sends, mine1, mine2, scaled, here, sems = refs[:3], refs[3], refs[4], refs[5], refs[6], refs[7]
    core, z = core_ref[0], z_ref[0]
    rows, wide = sends[0].shape
    part, half = wide // 2, mine1.shape[1]
    pairs = [(tokens, here)]
    for step, send in enumerate(sends, 1):
        at = pl.ds(pl.multiple_of(((z + step) % 4) * part, 128), part)
        for side, w in enumerate((gate, upward)):
            source = w.at[pl.ds(core * rows, rows), at]
            pairs.append((source, send.at[:, pl.ds(side * part, part)]))
    for w, mine in ((down1, mine1), (down2, mine2)):
        pairs.append((w.at[:, at_lane(core, half)], mine))
    copies = together(pairs, sems)
    copies[0].wait()
    scaled[...] = (here[...].astype(f32) * gain[...].astype(f32).reshape(1, -1)).astype(bf16)
    wait_for(copies[1:])


def message(core_ref, y_ref, branch, gain, here, tokens, gate, upward, out, picked, sems):
    core, y = core_ref[0], y_ref[0]
    width, cols = picked.shape
    each = cols // 16

    @pl.when(core == 0)
    def _():
        pltpu.make_async_copy(gate, picked, sems.at[16]).start()

    @pl.when(core == 1)
    def _():
        pltpu.make_async_copy(upward, picked, sems.at[16]).start()

    pairs = []
    for z in range(4):
        for x in range(4):
            source = tokens.at[pl.ds(x * 128 + 32 * z + 8 * y, 8), :]
            pairs.append((source, out.at[4 * z + x, pl.ds(each, 8), :]))
    copies = together(pairs, sems)
    wide = here[...].astype(f32)
    squares = lax.dot_general(
        jnp.ones((8, width), f32),
        wide * wide,
        (((1,), (1,)), ((), ())),
        precision=lax.Precision.HIGHEST,
        preferred_element_type=f32,
    )
    high = squares.astype(bf16).astype(f32)
    mid = (squares - high).astype(bf16).astype(f32)
    low = squares - high - mid
    row = lax.broadcasted_iota(jnp.int32, (8, width), 0)
    fixed = jnp.where(row == 0, branch[...].astype(f32), jnp.where(row == 1, gain[...].astype(f32), 0.0))
    blocks = []
    for x in range(4):
        at = slice(128 * x, 128 * x + 128)
        first = jnp.concatenate([high[:, at], mid[:, at]], 1)
        second = jnp.concatenate([low[:, at], jnp.zeros_like(low[:, at])], 1)
        blocks.append(jnp.where(row == 2, first, jnp.where(row == 3, second, fixed)).astype(bf16))
    pltpu.make_async_copy(gate, picked, sems.at[16]).wait()
    turned = picked[...].T
    for z in range(4):
        for x in range(4):
            to = 4 * z + x
            out[to, :each, :] = turned[to * each : (to + 1) * each, :]
            out[to, each + 8 :, :] = blocks[x]
    wait_for(copies)


def up_part(core_ref, x_ref, z_ref, first_x, gate, upward, *refs):
    xs, mine, other = refs[:3], refs[3:6], refs[6:9]
    own, sends, acc, whole, held, sems = refs[9], refs[10:13], refs[13], refs[14], refs[15], refs[16]
    core, x, z = core_ref[0], x_ref[0], z_ref[0]
    rows, wide = mine[0].shape
    part = wide // 2
    at = pl.ds(pl.multiple_of(z * part, 128), part)
    copies = [[]]
    for side, w in enumerate((gate, upward)):
        copies[0].append((w.at[:, at], whole.at[0, :, pl.ds(side * part, part)]))
    for step in range(3):
        here = (mine[step], whole.at[step + 1, pl.ds(core * rows, rows), :])
        there = (other[step], whole.at[step + 1, pl.ds((1 - core) * rows, rows), :])
        copies.append([here, there, (xs[step], held.at[step])])
    copies = [together(group, sems.at[step]) for step, group in enumerate(copies)]
    total = None
    for step in range(4):
        wait_for(copies[step])
        tokens = held[step - 1] if step else first_x[...]
        one = dot(tokens, whole[step], ((1,), (0,)))
        total = one if total is None else total + one
    acc[...] = total
    own[...] = acc[pl.ds(x * 128, 128), :]
    for step, send in enumerate(sends, 1):
        send[...] = acc[pl.ds(((x + step) % 4) * 128, 128), :].astype(bf16)


def down_part(core_ref, x_ref, own, a, b, c, side, w, *refs):
    mine, other, out, whole, small, sems = refs[:3], refs[3:6], refs[6], refs[7], refs[8], refs[9]
    core, x = core_ref[0], x_ref[0]
    rows, full = w.shape
    half = full // 2
    copies = [(side.at[:, pl.ds(rows, 16), :], small), (w, whole.at[pl.ds(x * rows, rows), :])]
    for step in range(1, 4):
        at = pl.ds(((x + 4 - step) % 4) * rows, rows)
        copies.append((mine[step - 1], whole.at[at, at_lane(core, half)]))
        copies.append((other[step - 1], whole.at[at, at_lane(1 - core, half)]))
    copies = together(copies, sems)
    both = own[...] + a[...].astype(f32) + b[...].astype(f32) + c[...].astype(f32)
    copies[0].wait()
    squares = jnp.sum(small[...].astype(f32), axis=0)[10:12]
    squares = squares[0:1, :128] + squares[0:1, 128:] + squares[1:2, :128]
    scale = lax.rsqrt(squares / full + epsilon)
    both = both * jnp.broadcast_to(scale, (8, 128)).T[:, :1]
    part = both.shape[1] // 2
    hidden = (silu(both[:, :part]) * both[:, part:]).astype(bf16)
    wait_for(copies[1:])
    out[...] = dot(hidden, whole[...], ((1,), (0,))).astype(bf16)


def join(got, side, send, small, sem):
    copy = pltpu.make_async_copy(side.at[:, pl.ds(side.shape[1] - 16, 16), :], small, sem)
    copy.start()
    total = jnp.sum(got[...].astype(f32), axis=0)
    copy.wait()
    blocks = [small[i].astype(f32) for i in range(16)]
    tokens, branch, gain = (jnp.concatenate([b[at] for b in blocks], 1) for at in (slice(0, 8), slice(8, 9), slice(9, 10)))
    middle = (residual_scale * tokens + 0.5 * branch * total).astype(bf16)
    mid = middle.astype(f32)
    square = jnp.mean(mid * mid, axis=1, keepdims=True)
    normed = (mid * lax.rsqrt(square + epsilon) * gain).astype(bf16)
    full = normed.shape[1]
    width = full // 16
    for x in range(4):
        for z in range(4):
            block = (4 * z + x) * width
            send[4 * x + z, :, :full] = normed
            send[4 * x + z, :, full:] = middle[:, block : block + width]


def finish(got, branch, send, out, middle, sems):
    count, rows = send.shape[:2]
    width = out.shape[2]
    pairs = [(send.at[:, :, pl.ds(send.shape[2] - width, width)], middle)]
    copies = together(pairs, sems)
    total = jnp.sum(got[...].astype(f32), axis=0)
    wait_for(copies)
    for j in range(count):
        at = slice(j * rows, (j + 1) * rows)
        mid = middle[j].astype(f32)
        value = (residual_scale * mid + 0.5 * branch[...].astype(f32) * total[at]).astype(bf16)
        for y in range(4):
            out[y, at, :] = value


def gated(core, tokens, sources, up, sems):
    blocks, rows, width = up.shape
    cols = rows // 8
    groups = sems.shape[0]
    each = blocks // groups
    pending = []
    for group in range(groups):
        pairs = []
        for w, first, slot, side in sources:
            begin = group * each - first
            if 0 <= begin < w.shape[0]:
                place = 1 - core if side else core
                to = up.at[pl.ds(group * each, each), pl.ds(slot * 2 * cols + place * cols, cols), :]
                pairs.append((w.at[pl.ds(begin, each), pl.ds(0, cols), :], to))
        pending.append(together(pairs, sems.at[group]))

    def finish():
        total = None
        for group in range(groups):
            wait_for(pending[group])
            for block in range(group * each, (group + 1) * each):
                part = dot(up[block], tokens[:, block * width : (block + 1) * width], ((1,), (1,)))
                total = part if total is None else total + part
        hidden = []
        for i in range(rows // (2 * cols)):
            gate = total[2 * i * cols : (2 * i + 1) * cols]
            hidden.append(silu(gate) * total[(2 * i + 1) * cols : (2 * i + 2) * cols])
        return jnp.concatenate(hidden, 0)

    return finish


def feed_forward(core_ref, got, w_down, *refs):
    ups, mine, other, out = refs[:14], refs[14:17], refs[17:20], refs[20]
    tokens, up, whole, up_sems, down_sems = refs[21:]
    core = core_ref[0]
    rows, full = w_down.shape
    half = full // 2
    blocks, _, width = up.shape
    sources = [(ups[0], 0, 0, 0), (ups[1], 0, 0, 1)]
    for i, w in enumerate(ups[2:]):
        sources.append((w, blocks // 2 * (i // 2 % 2), 1 + i // 4, i % 2))
    finish = gated(core, tokens, sources, up, up_sems)
    pairs = [(w_down, whole.at[pl.ds(0, rows), :])]
    for step in range(1, 4):
        at = pl.ds(step * rows, rows)
        pairs.append((mine[step - 1], whole.at[at, at_lane(core, half)]))
        pairs.append((other[step - 1], whole.at[at, at_lane(1 - core, half)]))
    copies = together(pairs, down_sems)
    for j in range(got.shape[0]):
        tokens[8 * j : 8 * j + 8, :] = got[j, :, :full]
    hidden = finish().T.astype(bf16)
    wait_for(copies)
    for block in range(blocks):
        lanes = slice(block * width, (block + 1) * width)
        out[block] = dot(hidden, whole[:, lanes], ((1,), (0,))).astype(bf16)


def shards(
    tokens,
    first_gain,
    first_gate,
    first_up,
    first_down,
    first_branch,
    second_gain,
    second_gate,
    second_up,
    second_down,
    second_branch,
):
    core, x, y, z = (lax.axis_index(name) for name in ("dp", "rx", "cb", "rz"))
    core_ref, x_ref, y_ref, z_ref = (i.astype(jnp.int32).reshape(1) for i in (core, x, y, z))
    n_tok, width = tokens.shape
    full = width * 16
    half = width // 2
    cols = first_gate.shape[1]
    part = cols // 4
    few = n_tok // 4
    w_half = jax.ShapeDtypeStruct((first_down.shape[0], full // 2), bf16)

    def kernel(body, ins, *outs, scratch=(), mib=16):
        call = pl.pallas_call(
            body,
            out_shape=list(outs) if len(outs) > 1 else outs[0],
            in_specs=ins,
            out_specs=[VMEM] * len(outs) if len(outs) > 1 else VMEM,
            scratch_shapes=list(scratch),
            compiler_params=pltpu.CompilerParams(vmem_limit_bytes=mib * 2**20),
        )

        def run(*args):
            kept = [pltpu.with_memory_space_constraint(a, pltpu.HBM) if spec is HBM else a for a, spec in zip(args, ins)]
            return call(*kept)

        return run

    dma = pltpu.SemaphoreType.DMA

    *w1, d1, d2, scaled = kernel(
        pack,
        [SMEM] * 2 + [VMEM] + [HBM] * 5,
        *[jax.ShapeDtypeStruct((half, 2 * part), bf16)] * 3,
        w_half,
        w_half,
        jax.ShapeDtypeStruct(tokens.shape, bf16),
        scratch=[pltpu.VMEM(tokens.shape, bf16), dma((9,))],
    )(core_ref, z_ref, first_gain, tokens, first_gate, first_up, first_down, second_down)
    w1 = [shifted(w, "rz", step) for step, w in enumerate(w1, 1)]
    x1 = [scaled] + [shifted(scaled, "rz", step) for step in (1, 2, 3)]
    w1_other = [other_core(w) for w in w1]

    side = kernel(
        message,
        [SMEM] * 2 + [VMEM] * 3 + [HBM] * 3,
        jax.ShapeDtypeStruct((16, cols // 16 + 16, width), bf16),
        scratch=[pltpu.VMEM((width, cols), bf16), dma((17,))],
    )(core_ref, y_ref, first_branch[None], second_gain[None], tokens, tokens, second_gate, second_up)
    side = exchange(side, ("rz", "rx"))
    d1 = [shifted(d1, "rx", step) for step in (1, 2, 3)]
    d2 = [shifted(d2, "cb", step) for step in (1, 2, 3)]
    d1_other = [other_core(w) for w in d1]
    d2_other = [other_core(w) for w in d2]

    def swapped(ws):
        return [other_core(w) for w in ws]

    low, high = side[:8, : cols // 16], side[8:, : cols // 16]
    low = [shifted(low, "cb", step) for step in (1, 3)]
    high = [shifted(high, "cb", step) for step in (1, 3)]
    far = [shifted(low[0], "cb", 1)]
    far += [shifted(high[1], "cb", 3)]
    own_other, *low_other = swapped([side, *low])
    high_other = swapped(high)
    far_other = swapped(far)
    v1 = [side, own_other, low[0], low_other[0], high[0], high_other[0]]
    v1 += [far[0], far_other[0], far[1], far_other[1], low[1], low_other[1], high[1], high_other[1]]

    own, *sends = kernel(
        up_part,
        [SMEM] * 3 + [VMEM] + [HBM] * 11,
        jax.ShapeDtypeStruct((few, 2 * part), f32),
        *[jax.ShapeDtypeStruct((few, 2 * part), bf16)] * 3,
        scratch=[
            pltpu.VMEM((n_tok, 2 * part), f32),
            pltpu.VMEM((4, width, 2 * part), bf16),
            pltpu.VMEM((3, n_tok, width), bf16),
            dma((4, 3)),
        ],
    )(core_ref, x_ref, z_ref, x1[0], first_gate, first_up, *x1[1:], *w1, *w1_other)
    got = [shifted(send, "rx", step) for step, send in enumerate(sends, 1)]
    partial = kernel(
        down_part,
        [SMEM] * 2 + [VMEM] * 4 + [HBM] * 8,
        pltpu.VMEM((few, full), bf16),
        scratch=[pltpu.VMEM((part, full), bf16), pltpu.VMEM((16, 16, width), bf16), dma((8,))],
    )(core_ref, x_ref, own, *got, side, first_down, *d1, *d1_other)
    got = exchange(partial.reshape(16, 8, full), ("rz", "cb"))
    send = kernel(
        join,
        [VMEM, HBM],
        jax.ShapeDtypeStruct((16, 8, full + width), bf16),
        scratch=[pltpu.VMEM((16, 16, width), bf16), dma(())],
    )(got, side)
    rows = exchange(send, ("rx", "rz"))
    partial = kernel(
        feed_forward,
        [SMEM, VMEM] + [HBM] * 2 + [ANY] + [HBM] * 18,
        pltpu.VMEM((16, few, width), bf16),
        scratch=[
            pltpu.VMEM((few, full), bf16),
            pltpu.VMEM((16, 2 * part, width), bf16),
            pltpu.VMEM((part, full), bf16),
            dma((4, 8)),
            dma((7,)),
        ],
        mib=24,
    )(core_ref, rows, second_down, *v1, *d2, *d2_other)
    partial, branch = lax.optimization_barrier((partial, second_branch[None]))
    got = exchange(partial, ("rz", "rx"))
    out = kernel(
        finish,
        [VMEM, VMEM, HBM],
        pltpu.VMEM((4, few, width), bf16),
        scratch=[pltpu.VMEM((16, 8, width), bf16), dma((1,))],
    )(got, branch, rows)
    out = exchange(out, "cb")
    return out.reshape(4, 16, 8, width).transpose(1, 0, 2, 3).reshape(n_tok, width)


def solution(mesh):
    fine = Mesh(mesh.devices.reshape(4, 4, 4, 2), ("rz", "rx", "cb", "dp"))
    ra = ("rz", "rx")
    vector, up, dn = P(ra), P(ra, "cb"), P(("cb", *ra), None)
    layer = (vector, up, up, dn, vector)
    return jax.shard_map(
        shards,
        mesh=fine,
        in_specs=(P("dp", ra), *layer, *layer),
        out_specs=P("dp", ra),
        check_vma=False,
    )
```

```python
import jax
import jax.numpy as jnp
from jax import lax
from jax.experimental import pallas as pl
from jax.experimental.pallas import tpu as pltpu
from jax.sharding import Mesh, PartitionSpec as P

epsilon = 1e-06
residual_scale = 0.25
f32 = jnp.float32
bf16 = jnp.bfloat16
VMEM = pl.BlockSpec(memory_space=pltpu.VMEM)
SMEM = pl.BlockSpec(memory_space=pltpu.SMEM)
HBM = pl.BlockSpec(memory_space=pltpu.HBM)
ANY = pl.BlockSpec(memory_space=pl.ANY)


def exchange(x, axes):
    return lax.all_to_all(x, axes, 0, 0, tiled=True)


def other_core(x):
    return lax.ppermute(x, "dp", [(0, 1), (1, 0)])


def shifted(x, axis, step):
    return lax.ppermute(x, axis, [(i, (i + step) % 4) for i in range(4)])


def dot(a, b, dims):
    return lax.dot_general(a, b, (dims, ((), ())), preferred_element_type=f32)


def silu(v):
    return v / (1.0 + jnp.exp(-v))


def at_lane(core, half):
    return pl.ds(pl.multiple_of(core * half, 128), half)


def together(pairs, sems):
    copies = [pltpu.make_async_copy(*pair, sems.at[i]) for i, pair in enumerate(pairs)]
    for copy in copies:
        copy.start()
    return copies


def wait_for(copies):
    for copy in copies:
        copy.wait()


def pack(core_ref, z_ref, gain, tokens, gate, upward, down1, down2, *refs):
    sends, mine1, mine2, scaled, here, sems = refs[:3], refs[3], refs[4], refs[5], refs[6], refs[7]
    core, z = core_ref[0], z_ref[0]
    rows, wide = sends[0].shape
    part, half = wide // 2, mine1.shape[1]
    pairs = [(tokens, here)]
    for step, send in enumerate(sends, 1):
        at = pl.ds(pl.multiple_of(((z + step) % 4) * part, 128), part)
        for side, w in enumerate((gate, upward)):
            source = w.at[pl.ds(core * rows, rows), at]
            pairs.append((source, send.at[:, pl.ds(side * part, part)]))
    for w, mine in ((down1, mine1), (down2, mine2)):
        pairs.append((w.at[:, at_lane(core, half)], mine))
    copies = together(pairs, sems)
    copies[0].wait()
    scaled[...] = (here[...].astype(f32) * gain[...].astype(f32).reshape(1, -1)).astype(bf16)
    wait_for(copies[1:])


def message(core_ref, y_ref, branch, gain, here, tokens, gate, upward, out, picked, sems):
    core, y = core_ref[0], y_ref[0]
    width, cols = picked.shape
    each = cols // 16

    @pl.when(core == 0)
    def _():
        pltpu.make_async_copy(gate, picked, sems.at[16]).start()

    @pl.when(core == 1)
    def _():
        pltpu.make_async_copy(upward, picked, sems.at[16]).start()

    pairs = []
    for z in range(4):
        for x in range(4):
            source = tokens.at[pl.ds(x * 128 + 32 * z + 8 * y, 8), :]
            pairs.append((source, out.at[4 * z + x, pl.ds(each, 8), :]))
    copies = together(pairs, sems)
    wide = here[...].astype(f32)
    squares = lax.dot_general(
        jnp.ones((8, width), f32),
        wide * wide,
        (((1,), (1,)), ((), ())),
        precision=lax.Precision.HIGHEST,
        preferred_element_type=f32,
    )
    high = squares.astype(bf16).astype(f32)
    mid = (squares - high).astype(bf16).astype(f32)
    low = squares - high - mid
    row = lax.broadcasted_iota(jnp.int32, (8, width), 0)
    fixed = jnp.where(row == 0, branch[...].astype(f32), jnp.where(row == 1, gain[...].astype(f32), 0.0))
    blocks = []
    for x in range(4):
        at = slice(128 * x, 128 * x + 128)
        first = jnp.concatenate([high[:, at], mid[:, at]], 1)
        second = jnp.concatenate([low[:, at], jnp.zeros_like(low[:, at])], 1)
        blocks.append(jnp.where(row == 2, first, jnp.where(row == 3, second, fixed)).astype(bf16))
    pltpu.make_async_copy(gate, picked, sems.at[16]).wait()
    turned = picked[...].T
    for z in range(4):
        for x in range(4):
            to = 4 * z + x
            out[to, :each, :] = turned[to * each : (to + 1) * each, :]
            out[to, each + 8 :, :] = blocks[x]
    wait_for(copies)


def up_part(core_ref, x_ref, z_ref, first_x, gate, upward, *refs):
    xs, mine, other = refs[:3], refs[3:6], refs[6:9]
    own, sends, acc, whole, held, sems = refs[9], refs[10:13], refs[13], refs[14], refs[15], refs[16]
    core, x, z = core_ref[0], x_ref[0], z_ref[0]
    rows, wide = mine[0].shape
    part = wide // 2
    at = pl.ds(pl.multiple_of(z * part, 128), part)
    copies = [[]]
    for side, w in enumerate((gate, upward)):
        copies[0].append((w.at[:, at], whole.at[0, :, pl.ds(side * part, part)]))
    for step in range(3):
        here = (mine[step], whole.at[step + 1, pl.ds(core * rows, rows), :])
        there = (other[step], whole.at[step + 1, pl.ds((1 - core) * rows, rows), :])
        copies.append([here, there, (xs[step], held.at[step])])
    copies = [together(group, sems.at[step]) for step, group in enumerate(copies)]
    total = None
    for step in range(4):
        wait_for(copies[step])
        tokens = held[step - 1] if step else first_x[...]
        one = dot(tokens, whole[step], ((1,), (0,)))
        total = one if total is None else total + one
    acc[...] = total
    own[...] = acc[pl.ds(x * 128, 128), :]
    for step, send in enumerate(sends, 1):
        send[...] = acc[pl.ds(((x + step) % 4) * 128, 128), :].astype(bf16)


def down_part(core_ref, x_ref, own, a, b, c, side, w, *refs):
    mine, other, out, whole, small, sems = refs[:3], refs[3:6], refs[6], refs[7], refs[8], refs[9]
    core, x = core_ref[0], x_ref[0]
    rows, full = w.shape
    half = full // 2
    copies = [(side.at[:, pl.ds(rows, 16), :], small), (w, whole.at[pl.ds(x * rows, rows), :])]
    for step in range(1, 4):
        at = pl.ds(((x + 4 - step) % 4) * rows, rows)
        copies.append((mine[step - 1], whole.at[at, at_lane(core, half)]))
        copies.append((other[step - 1], whole.at[at, at_lane(1 - core, half)]))
    copies = together(copies, sems)
    both = own[...] + a[...].astype(f32) + b[...].astype(f32) + c[...].astype(f32)
    copies[0].wait()
    squares = jnp.sum(small[...].astype(f32), axis=0)[10:12]
    squares = squares[0:1, :128] + squares[0:1, 128:] + squares[1:2, :128]
    scale = lax.rsqrt(squares / full + epsilon)
    both = both * jnp.broadcast_to(scale, (8, 128)).T[:, :1]
    part = both.shape[1] // 2
    hidden = (silu(both[:, :part]) * both[:, part:]).astype(bf16)
    wait_for(copies[1:])
    out[...] = dot(hidden, whole[...], ((1,), (0,))).astype(bf16)


def join(got, side, send, small, sem):
    copy = pltpu.make_async_copy(side.at[:, pl.ds(side.shape[1] - 16, 16), :], small, sem)
    copy.start()
    total = jnp.sum(got[...].astype(f32), axis=0)
    copy.wait()
    blocks = [small[i].astype(f32) for i in range(16)]
    tokens, branch, gain = (jnp.concatenate([b[at] for b in blocks], 1) for at in (slice(0, 8), slice(8, 9), slice(9, 10)))
    middle = (residual_scale * tokens + 0.5 * branch * total).astype(bf16)
    mid = middle.astype(f32)
    square = jnp.mean(mid * mid, axis=1, keepdims=True)
    normed = (mid * lax.rsqrt(square + epsilon) * gain).astype(bf16)
    full = normed.shape[1]
    width = full // 16
    for x in range(4):
        for z in range(4):
            block = (4 * z + x) * width
            send[4 * x + z, :, :full] = normed
            send[4 * x + z, :, full:] = middle[:, block : block + width]


def finish(got, branch, send, out, middle, sems):
    count, rows = send.shape[:2]
    width = out.shape[2]
    pairs = [(send.at[:, :, pl.ds(send.shape[2] - width, width)], middle)]
    copies = together(pairs, sems)
    total = jnp.sum(got[...].astype(f32), axis=0)
    wait_for(copies)
    for j in range(count):
        at = slice(j * rows, (j + 1) * rows)
        mid = middle[j].astype(f32)
        value = (residual_scale * mid + 0.5 * branch[...].astype(f32) * total[at]).astype(bf16)
        for y in range(4):
            out[y, at, :] = value


def gated(core, tokens, sources, up, sems):
    blocks, rows, width = up.shape
    cols = rows // 8
    groups = sems.shape[0]
    each = blocks // groups
    pending = []
    for group in range(groups):
        pairs = []
        for w, first, slot, side in sources:
            begin = group * each - first
            if 0 <= begin < w.shape[0]:
                place = 1 - core if side else core
                to = up.at[pl.ds(group * each, each), pl.ds(slot * 2 * cols + place * cols, cols), :]
                pairs.append((w.at[pl.ds(begin, each), pl.ds(0, cols), :], to))
        pending.append(together(pairs, sems.at[group]))

    def finish():
        total = None
        for group in range(groups):
            wait_for(pending[group])
            for block in range(group * each, (group + 1) * each):
                part = dot(up[block], tokens[:, block * width : (block + 1) * width], ((1,), (1,)))
                total = part if total is None else total + part
        hidden = []
        for i in range(rows // (2 * cols)):
            gate = total[2 * i * cols : (2 * i + 1) * cols]
            hidden.append(silu(gate) * total[(2 * i + 1) * cols : (2 * i + 2) * cols])
        return jnp.concatenate(hidden, 0)

    return finish


def feed_forward(core_ref, got, w_down, *refs):
    ups, mine, other, out = refs[:14], refs[14:17], refs[17:20], refs[20]
    tokens, up, whole, up_sems, down_sems = refs[21:]
    core = core_ref[0]
    rows, full = w_down.shape
    half = full // 2
    blocks, _, width = up.shape
    sources = [(ups[0], 0, 0, 0), (ups[1], 0, 0, 1)]
    for i, w in enumerate(ups[2:]):
        sources.append((w, blocks // 2 * (i // 2 % 2), 1 + i // 4, i % 2))
    finish = gated(core, tokens, sources, up, up_sems)
    pairs = [(w_down, whole.at[pl.ds(0, rows), :])]
    for step in range(1, 4):
        at = pl.ds(step * rows, rows)
        pairs.append((mine[step - 1], whole.at[at, at_lane(core, half)]))
        pairs.append((other[step - 1], whole.at[at, at_lane(1 - core, half)]))
    copies = together(pairs, down_sems)
    for j in range(got.shape[0]):
        tokens[8 * j : 8 * j + 8, :] = got[j, :, :full]
    hidden = finish().T.astype(bf16)
    wait_for(copies)
    for block in range(blocks):
        lanes = slice(block * width, (block + 1) * width)
        out[4 * (block % 4) + block // 4] = dot(hidden, whole[:, lanes], ((1,), (0,))).astype(bf16)


def shards(
    tokens,
    first_gain,
    first_gate,
    first_up,
    first_down,
    first_branch,
    second_gain,
    second_gate,
    second_up,
    second_down,
    second_branch,
):
    core, x, y, z = (lax.axis_index(name) for name in ("dp", "rx", "cb", "rz"))
    core_ref, x_ref, y_ref, z_ref = (i.astype(jnp.int32).reshape(1) for i in (core, x, y, z))
    n_tok, width = tokens.shape
    full = width * 16
    half = width // 2
    cols = first_gate.shape[1]
    part = cols // 4
    few = n_tok // 4
    w_half = jax.ShapeDtypeStruct((first_down.shape[0], full // 2), bf16)

    def kernel(body, ins, *outs, scratch=(), mib=16):
        call = pl.pallas_call(
            body,
            out_shape=list(outs) if len(outs) > 1 else outs[0],
            in_specs=ins,
            out_specs=[VMEM] * len(outs) if len(outs) > 1 else VMEM,
            scratch_shapes=list(scratch),
            compiler_params=pltpu.CompilerParams(vmem_limit_bytes=mib * 2**20),
        )

        def run(*args):
            kept = [pltpu.with_memory_space_constraint(a, pltpu.HBM) if spec is HBM else a for a, spec in zip(args, ins)]
            return call(*kept)

        return run

    dma = pltpu.SemaphoreType.DMA

    *w1, d1, d2, scaled = kernel(
        pack,
        [SMEM] * 2 + [VMEM] + [HBM] * 5,
        *[jax.ShapeDtypeStruct((half, 2 * part), bf16)] * 3,
        w_half,
        w_half,
        jax.ShapeDtypeStruct(tokens.shape, bf16),
        scratch=[pltpu.VMEM(tokens.shape, bf16), dma((9,))],
    )(core_ref, z_ref, first_gain, tokens, first_gate, first_up, first_down, second_down)
    w1 = [shifted(w, "rz", step) for step, w in enumerate(w1, 1)]
    x1 = [scaled] + [shifted(scaled, "rz", step) for step in (1, 2, 3)]
    w1_other = [other_core(w) for w in w1]

    side = kernel(
        message,
        [SMEM] * 2 + [VMEM] * 3 + [HBM] * 3,
        jax.ShapeDtypeStruct((16, cols // 16 + 16, width), bf16),
        scratch=[pltpu.VMEM((width, cols), bf16), dma((17,))],
    )(core_ref, y_ref, first_branch[None], second_gain[None], tokens, tokens, second_gate, second_up)
    side = exchange(side, ("rz", "rx"))
    d1 = [shifted(d1, "rx", step) for step in (1, 2, 3)]
    back, ahead = shifted(d2, "cb", 1), shifted(d2, "cb", 3)
    d2 = [back, shifted(d2, "cb", 2), ahead]
    d1_other = [other_core(w) for w in d1]
    d2_other = [other_core(w) for w in d2]

    def swapped(ws):
        return [other_core(w) for w in ws]

    low, high = side[:8, : cols // 16], side[8:, : cols // 16]
    low = [shifted(low, "cb", step) for step in (1, 3)]
    high = [shifted(high, "cb", step) for step in (1, 3)]
    far = [shifted(low[0], "cb", 1)]
    far += [shifted(high[1], "cb", 3)]
    own_other, *low_other = swapped([side, *low])
    high_other = swapped(high)
    far_other = swapped(far)
    v1 = [side, own_other, low[0], low_other[0], high[0], high_other[0]]
    v1 += [far[0], far_other[0], far[1], far_other[1], low[1], low_other[1], high[1], high_other[1]]

    own, *sends = kernel(
        up_part,
        [SMEM] * 3 + [VMEM] + [HBM] * 11,
        jax.ShapeDtypeStruct((few, 2 * part), f32),
        *[jax.ShapeDtypeStruct((few, 2 * part), bf16)] * 3,
        scratch=[
            pltpu.VMEM((n_tok, 2 * part), f32),
            pltpu.VMEM((4, width, 2 * part), bf16),
            pltpu.VMEM((3, n_tok, width), bf16),
            dma((4, 3)),
        ],
    )(core_ref, x_ref, z_ref, x1[0], first_gate, first_up, *x1[1:], *w1, *w1_other)
    got = [shifted(send, "rx", step) for step, send in enumerate(sends, 1)]
    partial = kernel(
        down_part,
        [SMEM] * 2 + [VMEM] * 4 + [HBM] * 8,
        pltpu.VMEM((few, full), bf16),
        scratch=[pltpu.VMEM((part, full), bf16), pltpu.VMEM((16, 16, width), bf16), dma((8,))],
    )(core_ref, x_ref, own, *got, side, first_down, *d1, *d1_other)
    got = exchange(partial.reshape(16, 8, full), ("rz", "cb"))
    send = kernel(
        join,
        [VMEM, HBM],
        jax.ShapeDtypeStruct((16, 8, full + width), bf16),
        scratch=[pltpu.VMEM((16, 16, width), bf16), dma(())],
    )(got, side)
    rows = exchange(send, ("rx", "rz"))
    partial = kernel(
        feed_forward,
        [SMEM, VMEM] + [HBM] * 2 + [ANY] + [HBM] * 18,
        pltpu.VMEM((16, few, width), bf16),
        scratch=[
            pltpu.VMEM((few, full), bf16),
            pltpu.VMEM((16, 2 * part, width), bf16),
            pltpu.VMEM((part, full), bf16),
            dma((4, 8)),
            dma((7,)),
        ],
        mib=24,
    )(core_ref, rows, second_down, *v1, *d2, *d2_other)
    partial, branch = lax.optimization_barrier((partial, second_branch[None]))
    got = exchange(partial, ("rx", "rz"))
    out = kernel(
        finish,
        [VMEM, VMEM, HBM],
        pltpu.VMEM((4, few, width), bf16),
        scratch=[pltpu.VMEM((16, 8, width), bf16), dma((1,))],
    )(got, branch, rows)
    out = exchange(out, "cb")
    return out.reshape(4, 16, 8, width).transpose(1, 0, 2, 3).reshape(n_tok, width)


def solution(mesh):
    fine = Mesh(mesh.devices.reshape(4, 4, 4, 2), ("rz", "rx", "cb", "dp"))
    ra = ("rz", "rx")
    vector, up, dn = P(ra), P(ra, "cb"), P(("cb", *ra), None)
    layer = (vector, up, up, dn, vector)
    return jax.shard_map(
        shards,
        mesh=fine,
        in_specs=(P("dp", ra), *layer, *layer),
        out_specs=P("dp", ra),
        check_vma=False,
    )
```
